256 devices in a mesh: ra: 32 (over z, y), cb: 8 (over x, core).
Axes of the slice: x: 4, y: 4, z: 8, core: 2. Of those that a mesh axis runs over, the one named last changes fastest.
Arguments:
- tokens: bfloat16 [128, 2048], P(None, 'ra'), may hold values from -6 to 6
- pre_gain: float32 [2, 2048], P(None, 'ra'), may hold values from 0.1 to 1.9
- post_gain: float32 [2, 2048], P(None, 'ra'), may hold values from 0.1 to 1.9
- gate_weight: bfloat16 [2, 2048, 5632], P(None, 'ra', 'cb'), may hold values from -0.125 to 0.125
- up_weight: bfloat16 [2, 2048, 5632], P(None, 'ra', 'cb'), may hold values from -0.125 to 0.125
- down_weight: bfloat16 [2, 5632, 2048], P(None, 'cb', 'ra'), may hold values from -0.078125 to 0.078125
Outputs:
- mixed: bfloat16 [128, 2048], P(None, 'ra')
The draws below stay inside these ranges and needn't reach their ends.
All inputs are finite; a program needn't handle non-finite values.
Results may differ from the reference program's by a relative error of at most 0.008.
Values may be sent and summed in bfloat16 or wider, within the bound.
No kernel may reach another device: no remote copies, remote signals or barrier semaphores. Data moves between devices by JAX's collectives and lax.ppermute only.
A program may use at most 64 MiB of HBM per device.

```python
import jax
import jax.numpy as jnp
from jax import lax

D = 2048
FF = 5632
LAYERS = 2
TOKENS = 128


def with_spikes(result, key, source, target, parts, factor):
    owner, partner = [(jnp.arange(result.shape[position]) // (result.shape[position] // parts)).reshape([-1 if axis == position else 1 for axis in range(result.ndim)]) for position in (source, target)]
    chosen = jax.random.permutation(key, parts)[partner]
    strong = (owner == chosen) | (owner == (partner + parts // 2) % parts)
    return jnp.where(strong, factor * result, result)


def level_of(stream_key, extent, shards, low, high):
    gain, own = 1.0, jax.random.fold_in(stream_key, 6)
    for position, parts in shards:
        draws = jnp.exp(jax.random.uniform(jax.random.fold_in(own, position), (parts,), jnp.float32, low / len(shards), high / len(shards)))
        gain = gain * jnp.repeat(draws, extent[position] // parts).reshape([-1 if axis == position else 1 for axis in range(len(extent))])
    return gain


def bell_draw(key, extent, spread, most, shards=(), held_as=jnp.bfloat16):
    loudness = level_of(key, extent, shards, -0.22, 0.18) if shards else 1.0
    result = jax.random.normal(key, extent, jnp.float32) * spread * loudness
    return jnp.minimum(jnp.maximum(result, -most), most).astype(held_as)


def heavy_noise(stream_key, extent, deviation, reach, cuts, heavy, kind=jnp.bfloat16):
    values = deviation * jax.random.normal(stream_key, extent, jnp.float32)
    if cuts:
        values = values * level_of(stream_key, extent, cuts, -0.22, 0.18)
    return jnp.clip(with_spikes(values, jax.random.fold_in(stream_key, 3), *heavy), -reach, reach).astype(kind)


def setup_inputs(seed: int = 0) -> dict:
    key_list = jax.random.split(jax.random.key(seed), 7)
    tokens = heavy_noise(key_list[0], (TOKENS, D), 1.0, 6.0, ((1, 32),), (1, 0, 32, 2.75))
    pre_gain = jnp.clip(1.0 + 0.18 * jax.random.normal(key_list[1], (LAYERS, D), jnp.float32), 0.1, 1.9)
    post_gain = jnp.clip(1.0 + 0.18 * jax.random.normal(key_list[2], (LAYERS, D), jnp.float32), 0.1, 1.9)
    gate_weight = bell_draw(key_list[3], (LAYERS, D, FF), D ** -0.5, 0.125, ((1, 32), (2, 8)))
    up_weight = bell_draw(key_list[4], (LAYERS, D, FF), D ** -0.5, 0.125, ((1, 32), (2, 8)))
    down_weight = bell_draw(key_list[5], (LAYERS, FF, D), FF ** -0.5, 0.078125, ((1, 8), (2, 32)))
    return {"tokens": tokens, "pre_gain": pre_gain, "post_gain": post_gain, "gate_weight": gate_weight, "up_weight": up_weight, "down_weight": down_weight}


epsilon = 1e-06
residual_scale = 0.25

def reference(tokens, pre_gain, post_gain, gate_weight, up_weight, down_weight):
    stream = tokens.astype(jnp.float32)
    for sublayer in range(LAYERS):
        scale_in = lax.rsqrt(lax.optimization_barrier(jnp.mean(stream * stream, axis=1, keepdims=True)) + epsilon)
        normed = (stream * scale_in * pre_gain[sublayer]).astype(jnp.bfloat16)
        gate_sum = jnp.dot(normed, gate_weight[sublayer], preferred_element_type=jnp.float32)
        up_sum = jnp.dot(normed, up_weight[sublayer], preferred_element_type=jnp.float32)
        hidden = (jax.nn.silu(gate_sum) * up_sum).astype(jnp.bfloat16)
        branch = jnp.dot(hidden, down_weight[sublayer], preferred_element_type=jnp.float32)
        scale_out = lax.rsqrt(lax.optimization_barrier(jnp.mean(branch * branch, axis=1, keepdims=True)) + epsilon)
        stream = residual_scale * stream + branch * scale_out * post_gain[sublayer]
    return stream.astype(jnp.bfloat16)
```

```python
import jax
import jax.numpy as jnp
from jax import lax
from jax.sharding import PartitionSpec as P

D = 2048
EPSILON = 1e-06
RESIDUAL = 0.25
CHUNK = 24
f32 = jnp.float32
bf16 = jnp.bfloat16


def exchange(tiles, axis):
    return lax.all_to_all(tiles, axis, 0, 0, tiled=True)


def to_all(tile, axis):
    n = lax.axis_size(axis)
    return exchange(jnp.broadcast_to(tile[None], (n, *tile.shape)), axis)


def project(weight, columns):
    return lax.dot_general(weight, columns, (((0,), (0,)), ((), ())), preferred_element_type=f32)


def project_wide(weight, columns):
    high = lax.reduce_precision(columns, 8, 7)
    both = project(weight, jnp.concatenate([high, columns - high], axis=1).astype(bf16))
    return both[:, : columns.shape[1]] + both[:, columns.shape[1] :]


def by_owner(part, n):
    part = jnp.pad(part, ((0, n * CHUNK - part.shape[0]), (0, 0)))
    return part.astype(bf16).reshape(n, CHUNK, part.shape[1])


def split_rows(sums):
    high = lax.reduce_precision(sums, 8, 7)
    rows = jnp.concatenate([high, sums - high]).astype(bf16)
    return jnp.pad(rows, ((0, 8 - rows.shape[0]), (0, 0)))


def total(sums):
    return jnp.sum(sums, axis=0, keepdims=True)


def per_device(tokens, pre_gain, post_gain, gate_weight, up_weight, down_weight):
    n = lax.axis_size("ra")
    start = tokens.T.astype(f32)
    width, ntok = start.shape
    pre = pre_gain[:, :, None]
    post = post_gain[:, :, None]

    first = start * pre[0]
    second = start * pre[1]
    parts = [
        by_owner(project_wide(w, x), n)
        for w, x in ((gate_weight[0], first), (up_weight[0], first), (gate_weight[1], second), (up_weight[1], second))
    ]
    stats = jnp.broadcast_to(split_rows(total(start * start))[None], (n, 8, ntok))
    got = jnp.sum(exchange(jnp.concatenate([*parts, stats], axis=1), "ra").astype(f32), axis=0)
    gate, up, old = got[:CHUNK], got[CHUNK : 2 * CHUNK], got[2 * CHUNK : 4 * CHUNK]
    squares = total(got[4 * CHUNK : 4 * CHUNK + 2])

    def branch_of(gate, up, sublayer):
        hidden = (jax.nn.silu(gate) * up).astype(bf16)
        hidden = to_all(hidden, "ra").reshape(n * CHUNK, ntok)[: down_weight.shape[1]]
        return jnp.sum(to_all(project(down_weight[sublayer], hidden), "cb"), axis=0)

    scale_in = lax.rsqrt(squares / D + EPSILON)
    branch = branch_of(gate * scale_in, up * scale_in, 0)

    gained = branch * post[0]
    fresh = gained * pre[1]
    parts = [by_owner(project_wide(w, fresh), n) for w in (gate_weight[1], up_weight[1])]
    stats = split_rows(jnp.concatenate([total(branch * branch), total(gained * gained), total(start * gained)]))
    stats = jnp.broadcast_to(stats[None], (n, 8, ntok))
    got = jnp.sum(exchange(jnp.concatenate([*parts, stats], axis=1), "ra").astype(f32), axis=0)
    sums = got[2 * CHUNK : 2 * CHUNK + 3] + got[2 * CHUNK + 3 : 2 * CHUNK + 6]
    branch_sq, gained_sq, cross = sums[0:1], sums[1:2], sums[2:3]
    scale_out = lax.rsqrt(branch_sq / D + EPSILON)
    squares = RESIDUAL * RESIDUAL * squares + 2.0 * RESIDUAL * scale_out * cross + scale_out * scale_out * gained_sq
    scale_in = lax.rsqrt(squares / D + EPSILON)
    both = (RESIDUAL * old + scale_out * got[: 2 * CHUNK]) * scale_in
    stream = RESIDUAL * start + gained * scale_out

    branch = branch_of(both[:CHUNK], both[CHUNK:], 1)
    branch_sq = jnp.sum(to_all(total(branch * branch), "ra"), axis=0)
    scale_out = lax.rsqrt(branch_sq / D + EPSILON)
    stream = RESIDUAL * stream + branch * post[1] * scale_out
    return stream.astype(bf16).T


def solution(mesh):
    return jax.shard_map(
        per_device,
        mesh=mesh,
        in_specs=(P(None, "ra"), P(None, "ra"), P(None, "ra"), P(None, "ra", "cb"), P(None, "ra", "cb"), P(None, "cb", "ra")),
        out_specs=P(None, "ra"),
        check_vma=False,
    )
```

```python
import jax
import jax.numpy as jnp
from jax import lax
from jax.sharding import Mesh
from jax.sharding import PartitionSpec as P

D = 2048
EPSILON = 1e-06
RESIDUAL = 0.25
CHUNK = 24
f32 = jnp.float32
bf16 = jnp.bfloat16


def exchange(tiles, axis):
    return lax.all_to_all(tiles, axis, 0, 0, tiled=True)


def to_all(tile, axis):
    n = lax.axis_size(axis)
    return exchange(jnp.broadcast_to(tile[None], (n, *tile.shape)), axis)


def project(weight, columns):
    return lax.dot_general(weight, columns, (((0,), (0,)), ((), ())), preferred_element_type=f32)


def project_wide(weight, columns):
    high = lax.reduce_precision(columns, 8, 7)
    both = project(weight, jnp.concatenate([high, columns - high], axis=1).astype(bf16))
    return both[:, : columns.shape[1]] + both[:, columns.shape[1] :]


def by_owner(part, n):
    part = jnp.pad(part, ((0, n * CHUNK - part.shape[0]), (0, 0)))
    return part.astype(bf16).reshape(n, CHUNK, part.shape[1])


def split_rows(sums):
    high = lax.reduce_precision(sums, 8, 7)
    rows = jnp.concatenate([high, sums - high]).astype(bf16)
    return jnp.pad(rows, ((0, 8 - rows.shape[0]), (0, 0)))


def total(sums):
    return jnp.sum(sums, axis=0, keepdims=True)


def per_device(tokens, pre_gain, post_gain, gate_weight, up_weight, down_weight):
    n = lax.axis_size("ra")
    start = tokens.T.astype(f32)
    width, ntok = start.shape
    pre = pre_gain[:, :, None]
    post = post_gain[:, :, None]

    first = start * pre[0]
    second = start * pre[1]
    parts = [
        by_owner(project_wide(w, x), n)
        for w, x in ((gate_weight[0], first), (up_weight[0], first), (gate_weight[1], second), (up_weight[1], second))
    ]
    stats = jnp.broadcast_to(split_rows(total(start * start))[None], (n, 8, ntok))
    got = jnp.sum(exchange(jnp.concatenate([*parts, stats], axis=1), "ra").astype(f32), axis=0)
    gate, up, old = got[:CHUNK], got[CHUNK : 2 * CHUNK], got[2 * CHUNK : 4 * CHUNK]
    squares = total(got[4 * CHUNK : 4 * CHUNK + 2])

    def branch_of(gate, up, sublayer):
        hidden = (jax.nn.silu(gate) * up).astype(bf16)
        hidden = to_all(hidden, "ra").reshape(n * CHUNK, ntok)[: down_weight.shape[1]]
        part = project(down_weight[sublayer], hidden)
        part = part + lax.ppermute(part, "core", [(0, 1), (1, 0)])
        return jnp.sum(to_all(part, "chip"), axis=0)

    scale_in = lax.rsqrt(squares / D + EPSILON)
    branch = branch_of(gate * scale_in, up * scale_in, 0)

    gained = branch * post[0]
    fresh = gained * pre[1]
    parts = [by_owner(project_wide(w, fresh), n) for w in (gate_weight[1], up_weight[1])]
    stats = split_rows(jnp.concatenate([total(branch * branch), total(gained * gained), total(start * gained)]))
    stats = jnp.broadcast_to(stats[None], (n, 8, ntok))
    got = jnp.sum(exchange(jnp.concatenate([*parts, stats], axis=1), "ra").astype(f32), axis=0)
    sums = got[2 * CHUNK : 2 * CHUNK + 3] + got[2 * CHUNK + 3 : 2 * CHUNK + 6]
    branch_sq, gained_sq, cross = sums[0:1], sums[1:2], sums[2:3]
    scale_out = lax.rsqrt(branch_sq / D + EPSILON)
    squares = RESIDUAL * RESIDUAL * squares + 2.0 * RESIDUAL * scale_out * cross + scale_out * scale_out * gained_sq
    scale_in = lax.rsqrt(squares / D + EPSILON)
    both = (RESIDUAL * old + scale_out * got[: 2 * CHUNK]) * scale_in
    stream = RESIDUAL * start + gained * scale_out

    branch = branch_of(both[:CHUNK], both[CHUNK:], 1)
    branch_sq = jnp.sum(to_all(total(branch * branch), "ra"), axis=0)
    scale_out = lax.rsqrt(branch_sq / D + EPSILON)
    stream = RESIDUAL * stream + branch * post[1] * scale_out
    return stream.astype(bf16).T


def solution(mesh):
    split = Mesh(mesh.devices.reshape(mesh.shape["ra"], mesh.shape["cb"] // 2, 2), ("ra", "chip", "core"))
    cb = ("chip", "core")
    return jax.shard_map(
        per_device,
        mesh=split,
        in_specs=(P(None, "ra"), P(None, "ra"), P(None, "ra"), P(None, "ra", cb), P(None, "ra", cb), P(None, cb, "ra")),
        out_specs=P(None, "ra"),
        check_vma=False,
    )
```

```python
import jax
import jax.numpy as jnp
from jax import lax
from jax.sharding import Mesh
from jax.sharding import PartitionSpec as P

D = 2048
EPSILON = 1e-06
RESIDUAL = 0.25
f32 = jnp.float32
bf16 = jnp.bfloat16


def exchange(tiles, axis):
    return lax.all_to_all(tiles, axis, 0, 0, tiled=True)


def to_all(tile, axis):
    n = lax.axis_size(axis)
    return exchange(jnp.broadcast_to(tile[None], (n, *tile.shape)), axis)


def project(weight, columns):
    return lax.dot_general(weight, columns, (((0,), (0,)), ((), ())), preferred_element_type=f32)


def project_wide(weight, columns):
    high = lax.reduce_precision(columns, 8, 7)
    both = project(weight, jnp.concatenate([high, columns - high], axis=1).astype(bf16))
    return both[:, : columns.shape[1]] + both[:, columns.shape[1] :]


def by_owner(part, n):
    return part.astype(bf16).reshape(n, part.shape[0] // n, part.shape[1])


def split_rows(sums):
    high = lax.reduce_precision(sums, 8, 7)
    rows = jnp.concatenate([high, sums - high]).astype(bf16)
    return rows


def total(sums):
    return jnp.sum(sums, axis=0, keepdims=True)


def per_device(tokens, pre_gain, post_gain, gate_weight, up_weight, down_weight):
    n = lax.axis_size("ra")
    size = gate_weight.shape[2] // n
    start = tokens.T.astype(f32)
    width, ntok = start.shape
    pre = pre_gain[:, :, None]
    post = post_gain[:, :, None]

    first = start * pre[0]
    second = start * pre[1]
    parts = [
        by_owner(project_wide(w, x), n)
        for w, x in ((gate_weight[0], first), (up_weight[0], first), (gate_weight[1], second), (up_weight[1], second))
    ]
    stats = jnp.broadcast_to(split_rows(total(start * start))[None], (n, 2, ntok))
    got = jnp.sum(exchange(jnp.concatenate([*parts, stats], axis=1), "ra").astype(f32), axis=0)
    gate, up, old = got[:size], got[size : 2 * size], got[2 * size : 4 * size]
    squares = total(got[4 * size : 4 * size + 2])

    def branch_of(gate, up, sublayer):
        hidden = (jax.nn.silu(gate) * up).astype(bf16)
        hidden = to_all(hidden, "ra").reshape(n * size, ntok)
        part = project(down_weight[sublayer], hidden)
        part = part + lax.ppermute(part, "core", [(0, 1), (1, 0)])
        return jnp.sum(to_all(part, "chip"), axis=0)

    scale_in = lax.rsqrt(squares / D + EPSILON)
    branch = branch_of(gate * scale_in, up * scale_in, 0)

    gained = branch * post[0]
    fresh = gained * pre[1]
    parts = [by_owner(project_wide(w, fresh), n) for w in (gate_weight[1], up_weight[1])]
    stats = jnp.concatenate([total(branch * branch), total(gained * gained), total(start * gained)]).astype(bf16)
    stats = jnp.broadcast_to(stats[None], (n, 3, ntok))
    got = jnp.sum(exchange(jnp.concatenate([*parts, stats], axis=1), "ra").astype(f32), axis=0)
    sums = got[2 * size : 2 * size + 3]
    branch_sq, gained_sq, cross = sums[0:1], sums[1:2], sums[2:3]
    scale_out = lax.rsqrt(branch_sq / D + EPSILON)
    squares = RESIDUAL * RESIDUAL * squares + 2.0 * RESIDUAL * scale_out * cross + scale_out * scale_out * gained_sq
    scale_in = lax.rsqrt(squares / D + EPSILON)
    both = (RESIDUAL * old + scale_out * got[: 2 * size]) * scale_in
    stream = RESIDUAL * start + gained * scale_out

    branch = branch_of(both[:size], both[size:], 1)
    branch_sq = jnp.sum(to_all(total(branch * branch), "ra"), axis=0)
    scale_out = lax.rsqrt(branch_sq / D + EPSILON)
    stream = RESIDUAL * stream + branch * post[1] * scale_out
    return stream.astype(bf16).T


def solution(mesh):
    split = Mesh(mesh.devices.reshape(mesh.shape["ra"], mesh.shape["cb"] // 2, 2), ("ra", "chip", "core"))
    cb = ("chip", "core")
    return jax.shard_map(
        per_device,
        mesh=split,
        in_specs=(P(None, "ra"), P(None, "ra"), P(None, "ra"), P(None, "ra", cb), P(None, "ra", cb), P(None, cb, "ra")),
        out_specs=P(None, "ra"),
        check_vma=False,
    )
```

```python
import jax
import jax.numpy as jnp
from jax import lax
from jax.experimental import pallas as pl
from jax.experimental.pallas import tpu as pltpu
from jax.sharding import Mesh
from jax.sharding import PartitionSpec as P

D = 2048
EPSILON = 1e-06
RESIDUAL = 0.25
f32 = jnp.float32
bf16 = jnp.bfloat16


def exchange(tiles, axis):
    return lax.all_to_all(tiles, axis, 0, 0, tiled=True)


def to_all(tile, axis):
    n = lax.axis_size(axis)
    return exchange(jnp.broadcast_to(tile[None], (n, *tile.shape)), axis)


def project(weight, columns):
    return lax.dot_general(weight, columns, (((0,), (0,)), ((), ())), preferred_element_type=f32)


def total(sums):
    return jnp.sum(sums, axis=0, keepdims=True)


def column(row):
    k = row.shape[1]
    same = lax.broadcasted_iota(jnp.int32, (k, k), 0) == lax.broadcasted_iota(jnp.int32, (k, k), 1)
    return jnp.sum(jnp.where(same, row, 0.0), axis=1, keepdims=True)


def stacked(columns):
    high = columns.astype(bf16)
    return jnp.concatenate([high, (columns - high.astype(f32)).astype(bf16)], axis=0)


def rows_of(values):
    at = lax.broadcasted_iota(jnp.int32, (8, values[0].shape[1]), 0)
    rows = jnp.zeros((8, values[0].shape[1]), f32)
    for i, value in enumerate(values):
        rows = jnp.where(at == i, value, rows)
    return rows


def multiply(flat_ref, j, weight, columns):
    twice = jnp.concatenate([weight, weight], axis=0)
    flat_ref[j] = lax.dot_general(twice, columns, (((0,), (0,)), ((), ())), preferred_element_type=f32)


def place(flat_ref, stage_ref, last, owners):
    count, width = flat_ref.shape[:2]
    size = width // stage_ref.shape[0]
    for i in owners:
        for j in range(count):
            stage_ref[i, j * size : (j + 1) * size] = flat_ref[j, i * size : (i + 1) * size]
        stage_ref[i, count * size : count * size + last.shape[0]] = last


def first_kernel(*refs):
    sources, (out_ref, flat_ref, stage_ref, tiles_ref, *held, in_sems, out_sems) = refs[:4], refs[4:]
    copies = [pltpu.make_async_copy(sources[i], held[i], in_sems.at[i]) for i in range(4)]
    for copy in copies:
        copy.start()
    tokens_ref, pre_ref, gate_ref, up_ref = held
    copies[0].wait()
    copies[1].wait()
    start = tokens_ref[...].astype(f32)
    squares = total(start * start)
    high = squares.astype(bf16).astype(f32)
    sums = rows_of([high, squares - high])
    columns = [stacked(start * column(pre_ref[sublayer : sublayer + 1])) for sublayer in range(2)]
    for k, ref in enumerate((gate_ref, up_ref)):
        copies[2 + k].wait()
        for sublayer in range(2):
            multiply(flat_ref, 2 * sublayer + k, ref[sublayer], columns[sublayer])
    n, groups = tiles_ref.shape[0], out_sems.shape[0]
    writes = []
    for g in range(groups):
        part = slice(g * n // groups, (g + 1) * n // groups)
        place(flat_ref, stage_ref, sums, range(part.start, part.stop))
        tiles_ref[part] = stage_ref[part].astype(bf16)
        writes.append(pltpu.make_async_copy(tiles_ref.at[part], out_ref.at[part], out_sems.at[g]))
        writes[-1].start()
    for write in writes:
        write.wait()


def first_tiles(n, *operands):
    width, ntok = operands[-1].shape[2], operands[0].shape[1]
    rows = 4 * (width // n) + 8
    hbm = pl.BlockSpec(memory_space=pltpu.HBM)
    return pl.pallas_call(
        first_kernel,
        out_shape=jax.ShapeDtypeStruct((n, rows, ntok), bf16),
        in_specs=[hbm] * 4,
        out_specs=hbm,
        scratch_shapes=[
            pltpu.VMEM((4, width, ntok), f32),
            pltpu.VMEM((n, rows, ntok), f32),
            pltpu.VMEM((n, rows, ntok), bf16),
            *[pltpu.VMEM(x.shape, x.dtype) for x in operands],
            pltpu.SemaphoreType.DMA((4,)),
            pltpu.SemaphoreType.DMA((4,)),
        ],
    )(*operands)


def second_kernel(parts_ref, tokens_ref, pre_ref, post_ref, gate_ref, up_ref, out_ref, gained_ref, last_ref, flat_ref, stage_ref):
    start = tokens_ref[...].astype(f32)
    branch = parts_ref[0]
    for i in range(1, parts_ref.shape[0]):
        branch = branch + parts_ref[i]
    gained = branch * column(post_ref[0:1])
    gained_ref[...] = gained
    last_ref[...] = jnp.broadcast_to(column(post_ref[1:2]), gained.shape)
    columns = stacked(gained * column(pre_ref[1:2]))
    sums = rows_of([total(branch * branch), total(gained * gained), total(start * gained)])[:4]
    for j, ref in enumerate((gate_ref, up_ref)):
        multiply(flat_ref, j, ref[1], columns)
    place(flat_ref, stage_ref, sums, range(out_ref.shape[0]))
    out_ref[...] = stage_ref[...].astype(bf16)


def second_tiles(n, *operands):
    width, ntok = operands[-1].shape[2], operands[1].shape[1]
    rows = 2 * (width // n) + 4
    vmem = pl.BlockSpec(memory_space=pltpu.VMEM)
    return pl.pallas_call(
        second_kernel,
        out_shape=[jax.ShapeDtypeStruct((n, rows, ntok), bf16), *[jax.ShapeDtypeStruct(operands[1].shape, f32)] * 2],
        in_specs=[vmem] * len(operands),
        out_specs=[vmem] * 3,
        scratch_shapes=[pltpu.VMEM((2, width, ntok), f32), pltpu.VMEM((n, rows, ntok), f32)],
        compiler_params=pltpu.CompilerParams(vmem_limit_bytes=12 * 2**20),
    )(*operands)


def per_device(tokens, pre_gain, post_gain, gate_weight, up_weight, down_weight):
    n = lax.axis_size("ra")
    size = gate_weight.shape[2] // n
    turned = tokens.T
    start = turned.astype(f32)
    ntok = start.shape[1]

    tiles = first_tiles(n, turned, pre_gain, gate_weight, up_weight)
    got = jnp.sum(exchange(tiles, "ra").astype(f32), axis=0)
    gate, up, old = got[:size], got[size : 2 * size], got[2 * size : 4 * size]
    squares = total(got[4 * size : 4 * size + 2])

    def branch_of(gate, up, sublayer):
        hidden = (jax.nn.silu(gate) * up).astype(bf16)
        hidden = to_all(hidden, "ra").reshape(n * size, ntok)
        part = project(down_weight[sublayer], hidden)
        part = part + lax.ppermute(part, "core", [(0, 1), (1, 0)])
        return to_all(part, "chip")

    scale_in = lax.rsqrt(squares / D + EPSILON)
    parts = branch_of(gate * scale_in, up * scale_in, 0)
    tiles, gained, last = second_tiles(n, parts, turned, pre_gain, post_gain, gate_weight, up_weight)
    got = jnp.sum(exchange(tiles, "ra").astype(f32), axis=0)
    sums = got[2 * size : 2 * size + 3]
    branch_sq, gained_sq, cross = sums[0:1], sums[1:2], sums[2:3]
    scale_out = lax.rsqrt(branch_sq / D + EPSILON)
    squares = RESIDUAL * RESIDUAL * squares + 2.0 * RESIDUAL * scale_out * cross + scale_out * scale_out * gained_sq
    scale_in = lax.rsqrt(squares / D + EPSILON)
    both = (RESIDUAL * old + scale_out * got[: 2 * size]) * scale_in
    stream = RESIDUAL * start + gained * scale_out

    branch = jnp.sum(branch_of(both[:size], both[size:], 1), axis=0)
    branch_sq = jnp.sum(to_all(total(branch * branch), "ra"), axis=0)
    scale_out = lax.rsqrt(branch_sq / D + EPSILON)
    stream = RESIDUAL * stream + branch * last * scale_out
    return stream.astype(bf16).T


def solution(mesh):
    split = Mesh(mesh.devices.reshape(mesh.shape["ra"], mesh.shape["cb"] // 2, 2), ("ra", "chip", "core"))
    cb = ("chip", "core")
    return jax.shard_map(
        per_device,
        mesh=split,
        in_specs=(P(None, "ra"), P(None, "ra"), P(None, "ra"), P(None, "ra", cb), P(None, "ra", cb), P(None, cb, "ra")),
        out_specs=P(None, "ra"),
        check_vma=False,
    )
```

```python
import jax
import jax.numpy as jnp
from jax import lax
from jax.experimental import pallas as pl
from jax.experimental.pallas import tpu as pltpu
from jax.sharding import PartitionSpec as P

D = 2048
EPSILON = 1e-06
RESIDUAL = 0.25
f32 = jnp.float32
bf16 = jnp.bfloat16


def exchange(tiles, axis):
    return lax.all_to_all(tiles, axis, 0, 0, tiled=True)


def to_all(tile, axis):
    n = lax.axis_size(axis)
    return exchange(jnp.broadcast_to(tile[None], (n, *tile.shape)), axis)


def sum_over(part, axis):
    width = part.shape[0]
    top = jnp.maximum(jnp.max(jnp.abs(part), axis=0, keepdims=True), 1e-30)
    power = jnp.floor(jnp.log2(top))
    tile = jnp.concatenate([part * jnp.exp2(-power), jnp.broadcast_to(power, (8, part.shape[1]))])
    got = to_all(tile.astype(jnp.float16), axis).astype(f32)
    return jnp.sum(got[:, :width] * jnp.exp2(got[:, width : width + 1]), axis=0)


def project(weight, columns):
    return lax.dot_general(weight, columns, (((0,), (0,)), ((), ())), preferred_element_type=f32)


def total(sums):
    return jnp.sum(sums, axis=0, keepdims=True)


def column(row):
    k = row.shape[1]
    same = lax.broadcasted_iota(jnp.int32, (k, k), 0) == lax.broadcasted_iota(jnp.int32, (k, k), 1)
    return jnp.sum(jnp.where(same, row, 0.0), axis=1, keepdims=True)


def stacked(columns):
    high = columns.astype(bf16)
    return jnp.concatenate([high, (columns - high.astype(f32)).astype(bf16)], axis=0)


def rows_of(values):
    at = lax.broadcasted_iota(jnp.int32, (8, values[0].shape[1]), 0)
    rows = jnp.zeros((8, values[0].shape[1]), f32)
    for i, value in enumerate(values):
        rows = jnp.where(at == i, value, rows)
    return rows


def multiply(flat_ref, j, weight, columns):
    twice = jnp.concatenate([weight, weight], axis=0)
    flat_ref[j] = lax.dot_general(twice, columns, (((0,), (0,)), ((), ())), preferred_element_type=f32)


def place(flat_ref, stage_ref, last, owners):
    count, width = flat_ref.shape[:2]
    size = width // stage_ref.shape[0]
    for i in owners:
        for j in range(count):
            stage_ref[i, j * size : (j + 1) * size] = flat_ref[j, i * size : (i + 1) * size]
        stage_ref[i, count * size : count * size + last.shape[0]] = last


def first_kernel(*refs):
    sources, (out_ref, flat_ref, stage_ref, tiles_ref, *held, in_sems, out_sems) = refs[:4], refs[4:]
    copies = [pltpu.make_async_copy(sources[i], held[i], in_sems.at[i]) for i in range(4)]
    for copy in copies:
        copy.start()
    tokens_ref, pre_ref, gate_ref, up_ref = held
    copies[0].wait()
    copies[1].wait()
    start = tokens_ref[...].astype(f32)
    squares = total(start * start)
    high = squares.astype(bf16).astype(f32)
    sums = rows_of([high, squares - high])
    columns = [stacked(start * column(pre_ref[sublayer : sublayer + 1])) for sublayer in range(2)]
    for k, ref in enumerate((gate_ref, up_ref)):
        copies[2 + k].wait()
        for sublayer in range(2):
            multiply(flat_ref, 2 * sublayer + k, ref[sublayer], columns[sublayer])
    n, groups = tiles_ref.shape[0], out_sems.shape[0]
    writes = []
    for g in range(groups):
        part = slice(g * n // groups, (g + 1) * n // groups)
        place(flat_ref, stage_ref, sums, range(part.start, part.stop))
        tiles_ref[part] = stage_ref[part].astype(bf16)
        writes.append(pltpu.make_async_copy(tiles_ref.at[part], out_ref.at[part], out_sems.at[g]))
        writes[-1].start()
    for write in writes:
        write.wait()


def first_tiles(n, *operands):
    width, ntok = operands[-1].shape[2], operands[0].shape[1]
    rows = 4 * (width // n) + 8
    hbm = pl.BlockSpec(memory_space=pltpu.HBM)
    return pl.pallas_call(
        first_kernel,
        out_shape=jax.ShapeDtypeStruct((n, rows, ntok), bf16),
        in_specs=[hbm] * 4,
        out_specs=hbm,
        scratch_shapes=[
            pltpu.VMEM((4, width, ntok), f32),
            pltpu.VMEM((n, rows, ntok), f32),
            pltpu.VMEM((n, rows, ntok), bf16),
            *[pltpu.VMEM(x.shape, x.dtype) for x in operands],
            pltpu.SemaphoreType.DMA((4,)),
            pltpu.SemaphoreType.DMA((4,)),
        ],
    )(*operands)


def second_kernel(branch_ref, tokens_ref, pre_ref, post_ref, gate_ref, up_ref, out_ref, gained_ref, last_ref, flat_ref, stage_ref):
    start = tokens_ref[...].astype(f32)
    branch = branch_ref[...]
    gained = branch * column(post_ref[0:1])
    gained_ref[...] = gained
    last_ref[...] = jnp.broadcast_to(column(post_ref[1:2]), gained.shape)
    columns = stacked(gained * column(pre_ref[1:2]))
    sums = rows_of([total(branch * branch), total(gained * gained), total(start * gained)])[:4]
    for j, ref in enumerate((gate_ref, up_ref)):
        multiply(flat_ref, j, ref[1], columns)
    place(flat_ref, stage_ref, sums, range(out_ref.shape[0]))
    out_ref[...] = stage_ref[...].astype(bf16)


def second_tiles(n, *operands):
    width, ntok = operands[-1].shape[2], operands[1].shape[1]
    rows = 2 * (width // n) + 4
    vmem = pl.BlockSpec(memory_space=pltpu.VMEM)
    return pl.pallas_call(
        second_kernel,
        out_shape=[jax.ShapeDtypeStruct((n, rows, ntok), bf16), *[jax.ShapeDtypeStruct(operands[1].shape, f32)] * 2],
        in_specs=[vmem] * len(operands),
        out_specs=[vmem] * 3,
        scratch_shapes=[pltpu.VMEM((2, width, ntok), f32), pltpu.VMEM((n, rows, ntok), f32)],
        compiler_params=pltpu.CompilerParams(vmem_limit_bytes=12 * 2**20),
    )(*operands)


def per_device(tokens, pre_gain, post_gain, gate_weight, up_weight, down_weight):
    n = lax.axis_size("ra")
    size = gate_weight.shape[2] // n
    turned = tokens.T
    start = turned.astype(f32)
    ntok = start.shape[1]

    tiles = first_tiles(n, turned, pre_gain, gate_weight, up_weight)
    got = jnp.sum(exchange(tiles, "ra").astype(f32), axis=0)
    gate, up, old = got[:size], got[size : 2 * size], got[2 * size : 4 * size]
    squares = total(got[4 * size : 4 * size + 2])

    def branch_of(gate, up, sublayer):
        hidden = (jax.nn.silu(gate) * up).astype(bf16)
        hidden = to_all(hidden, "ra").reshape(n * size, ntok)
        return sum_over(project(down_weight[sublayer], hidden), "cb")

    scale_in = lax.rsqrt(squares / D + EPSILON)
    branch = branch_of(gate * scale_in, up * scale_in, 0)
    tiles, gained, last = second_tiles(n, branch, turned, pre_gain, post_gain, gate_weight, up_weight)
    got = jnp.sum(exchange(tiles, "ra").astype(f32), axis=0)
    sums = got[2 * size : 2 * size + 3]
    branch_sq, gained_sq, cross = sums[0:1], sums[1:2], sums[2:3]
    scale_out = lax.rsqrt(branch_sq / D + EPSILON)
    squares = RESIDUAL * RESIDUAL * squares + 2.0 * RESIDUAL * scale_out * cross + scale_out * scale_out * gained_sq
    scale_in = lax.rsqrt(squares / D + EPSILON)
    both = (RESIDUAL * old + scale_out * got[: 2 * size]) * scale_in
    stream = RESIDUAL * start + gained * scale_out

    branch = branch_of(both[:size], both[size:], 1)
    branch_sq = jnp.sum(to_all(total(branch * branch), "ra"), axis=0)
    scale_out = lax.rsqrt(branch_sq / D + EPSILON)
    stream = RESIDUAL * stream + branch * last * scale_out
    return stream.astype(bf16).T


def solution(mesh):
    return jax.shard_map(
        per_device,
        mesh=mesh,
        in_specs=(P(None, "ra"), P(None, "ra"), P(None, "ra"), P(None, "ra", "cb"), P(None, "ra", "cb"), P(None, "cb", "ra")),
        out_specs=P(None, "ra"),
        check_vma=False,
    )
```

```python
import jax
import jax.numpy as jnp
from jax import lax
from jax.experimental import pallas as pl
from jax.experimental.pallas import tpu as pltpu
from jax.sharding import Mesh
from jax.sharding import PartitionSpec as P

D = 2048
EPSILON = 1e-06
RESIDUAL = 0.25
f32 = jnp.float32
bf16 = jnp.bfloat16


def exchange(tiles, axis):
    return lax.all_to_all(tiles, axis, 0, 0, tiled=True)


def to_all(tile, axis):
    n = lax.axis_size(axis)
    return exchange(jnp.broadcast_to(tile[None], (n, *tile.shape)), axis)


def swapped(array):
    return lax.ppermute(array, "core", [(0, 1), (1, 0)])


def project(weight, columns):
    return lax.dot_general(weight, columns, (((0,), (0,)), ((), ())), preferred_element_type=f32)


def total(sums):
    return jnp.sum(sums, axis=0, keepdims=True)


def column(row):
    k = row.shape[1]
    same = lax.broadcasted_iota(jnp.int32, (k, k), 0) == lax.broadcasted_iota(jnp.int32, (k, k), 1)
    return jnp.sum(jnp.where(same, row, 0.0), axis=1, keepdims=True)


def stacked(columns):
    left = lax.broadcasted_iota(jnp.int32, columns.shape, 1) < columns.shape[1] // 2
    high = columns.astype(bf16).astype(f32)
    parts = [jnp.where(mask, part, 0.0) for part in (high, columns - high) for mask in (left, jnp.logical_not(left))]
    return jnp.concatenate(parts, axis=0).astype(bf16)


def my_half(columns):
    half = columns.shape[1] // 2
    right = lax.broadcasted_iota(jnp.int32, columns.shape, 1) >= half
    mine = right == (lax.axis_index("core") == 1)
    return jnp.where(mine, columns, pltpu.roll(columns, half, 1))


def rows_of(values):
    at = lax.broadcasted_iota(jnp.int32, (8, values[0].shape[1]), 0)
    rows = jnp.zeros((8, values[0].shape[1]), f32)
    for i, value in enumerate(values):
        rows = jnp.where(at == i, value, rows)
    return rows


def multiply(flat_ref, j, mine, other, columns):
    weights = jnp.concatenate([mine, other, mine, other], axis=0)
    flat_ref[j] = lax.dot_general(weights, columns, (((0,), (0,)), ((), ())), preferred_element_type=f32)


def place(flat_ref, stage_ref, last, owners):
    count, width = flat_ref.shape[:2]
    size = width // stage_ref.shape[0]
    for i in owners:
        for j in range(count):
            stage_ref[i, j * size : (j + 1) * size] = flat_ref[j, i * size : (i + 1) * size]
        stage_ref[i, count * size : count * size + last.shape[0]] = last


def first_kernel(*refs):
    sources, (out_ref, flat_ref, stage_ref, tiles_ref, *held, in_sems, out_sems) = refs[:6], refs[6:]
    copies = [pltpu.make_async_copy(sources[i], held[i], in_sems.at[i]) for i in range(6)]
    for copy in copies:
        copy.start()
    tokens_ref, pre_ref, *weights = held
    copies[0].wait()
    copies[1].wait()
    start = my_half(tokens_ref[...].astype(f32))
    squares = total(start * start)
    high = squares.astype(bf16).astype(f32)
    sums = rows_of([high, squares - high])
    columns = [stacked(start * column(pre_ref[sublayer : sublayer + 1])) for sublayer in range(2)]
    for k in range(2):
        copies[2 + k].wait()
        copies[4 + k].wait()
        for sublayer in range(2):
            multiply(flat_ref, 2 * sublayer + k, weights[k][sublayer], weights[2 + k][sublayer], columns[sublayer])
    n, groups = tiles_ref.shape[0], out_sems.shape[0]
    writes = []
    for g in range(groups):
        part = slice(g * n // groups, (g + 1) * n // groups)
        place(flat_ref, stage_ref, sums, range(part.start, part.stop))
        tiles_ref[part] = stage_ref[part].astype(bf16)
        writes.append(pltpu.make_async_copy(tiles_ref.at[part], out_ref.at[part], out_sems.at[g]))
        writes[-1].start()
    for write in writes:
        write.wait()


def first_tiles(n, *operands):
    width, ntok = operands[-1].shape[2], operands[0].shape[1]
    rows = 4 * (width // n) + 8
    hbm = pl.BlockSpec(memory_space=pltpu.HBM)
    return pl.pallas_call(
        first_kernel,
        out_shape=jax.ShapeDtypeStruct((n, rows, ntok), bf16),
        in_specs=[hbm] * 6,
        out_specs=hbm,
        scratch_shapes=[
            pltpu.VMEM((4, width, ntok), f32),
            pltpu.VMEM((n, rows, ntok), f32),
            pltpu.VMEM((n, rows, ntok), bf16),
            *[pltpu.VMEM(x.shape, x.dtype) for x in operands],
            pltpu.SemaphoreType.DMA((6,)),
            pltpu.SemaphoreType.DMA((4,)),
        ],
    )(*operands)


def second_kernel(branch_ref, tokens_ref, pre_ref, post_ref, gate_ref, up_ref, gate2_ref, up2_ref, *refs):
    out_ref, start_ref, gained_ref, last_ref, flat_ref, stage_ref = refs
    start = my_half(tokens_ref[...].astype(f32))
    start_ref[...] = start
    branch = branch_ref[...]
    gained = branch * column(post_ref[0:1])
    gained_ref[...] = gained
    last_ref[...] = jnp.broadcast_to(column(post_ref[1:2]), gained.shape)
    columns = stacked(gained * column(pre_ref[1:2]))
    sums = rows_of([total(branch * branch), total(gained * gained), total(start * gained)])[:4]
    multiply(flat_ref, 0, gate_ref[1], gate2_ref[1], columns)
    multiply(flat_ref, 1, up_ref[1], up2_ref[1], columns)
    place(flat_ref, stage_ref, sums, range(out_ref.shape[0]))
    out_ref[...] = stage_ref[...].astype(bf16)


def second_tiles(n, *operands):
    width, ntok = operands[-1].shape[2], operands[1].shape[1]
    rows = 2 * (width // n) + 4
    vmem = pl.BlockSpec(memory_space=pltpu.VMEM)
    return pl.pallas_call(
        second_kernel,
        out_shape=[jax.ShapeDtypeStruct((n, rows, ntok), bf16), *[jax.ShapeDtypeStruct(operands[1].shape, f32)] * 3],
        in_specs=[vmem] * len(operands),
        out_specs=[vmem] * 4,
        scratch_shapes=[pltpu.VMEM((2, width, ntok), f32), pltpu.VMEM((n, rows, ntok), f32)],
        compiler_params=pltpu.CompilerParams(vmem_limit_bytes=12 * 2**20),
    )(*operands)


def per_device(tokens, pre_gain, post_gain, gate_weight, up_weight, down_weight):
    n = lax.axis_size("ra")
    size = gate_weight.shape[2] // n
    turned = tokens.T
    ntok = turned.shape[1]
    half = ntok // 2
    weights = gate_weight, up_weight, swapped(gate_weight), swapped(up_weight)
    other_down = swapped(down_weight)

    tiles = first_tiles(n, turned, pre_gain, *weights)
    got = jnp.sum(exchange(tiles, "ra").astype(f32), axis=0)
    gate, up, old = got[:size], got[size : 2 * size], got[2 * size : 4 * size]
    squares = total(got[4 * size : 4 * size + 2])

    def branch_of(gate, up, sublayer):
        hidden = (jax.nn.silu(gate) * up).astype(bf16)
        hidden = to_all(hidden, "ra").reshape(n * size, ntok)
        part = project(down_weight[sublayer], hidden)[:, :half] + project(other_down[sublayer], hidden)[:, half:]
        middle = part.shape[0] // 2
        tile = jnp.concatenate([part[:middle], part[middle:]], axis=1)
        tile = jnp.sum(to_all(tile, "chip"), axis=0)
        branch = jnp.concatenate([tile[:, :half], tile[:, half:]])
        return jnp.concatenate([branch, branch], axis=1)

    scale_in = lax.rsqrt(squares / D + EPSILON)
    branch = branch_of(gate * scale_in, up * scale_in, 0)
    tiles, start, gained, last = second_tiles(n, branch, turned, pre_gain, post_gain, *weights)
    got = jnp.sum(exchange(tiles, "ra").astype(f32), axis=0)
    sums = got[2 * size : 2 * size + 3]
    branch_sq, gained_sq, cross = sums[0:1], sums[1:2], sums[2:3]
    scale_out = lax.rsqrt(branch_sq / D + EPSILON)
    squares = RESIDUAL * RESIDUAL * squares + 2.0 * RESIDUAL * scale_out * cross + scale_out * scale_out * gained_sq
    scale_in = lax.rsqrt(squares / D + EPSILON)
    both = (RESIDUAL * old + scale_out * got[: 2 * size]) * scale_in
    stream = RESIDUAL * start + gained * scale_out

    branch = branch_of(both[:size], both[size:], 1)
    branch_sq = jnp.sum(to_all(total(branch * branch), "ra"), axis=0)
    scale_out = lax.rsqrt(branch_sq / D + EPSILON)
    stream = (RESIDUAL * stream + branch * last * scale_out).astype(bf16)
    right = lax.broadcasted_iota(jnp.int32, stream.shape, 1) >= half
    return jnp.where(right == (lax.axis_index("core") == 1), stream, swapped(stream)).T


def solution(mesh):
    split = Mesh(mesh.devices.reshape(mesh.shape["ra"], mesh.shape["cb"] // 2, 2), ("ra", "chip", "core"))
    cb = ("chip", "core")
    return jax.shard_map(
        per_device,
        mesh=split,
        in_specs=(P(None, "ra"), P(None, "ra"), P(None, "ra"), P(None, "ra", cb), P(None, "ra", cb), P(None, cb, "ra")),
        out_specs=P(None, "ra"),
        check_vma=False,
    )
```

```python
import jax
import jax.numpy as jnp
from jax import lax
from jax.experimental import pallas as pl
from jax.experimental.pallas import tpu as pltpu
from jax.sharding import Mesh
from jax.sharding import PartitionSpec as P

D = 2048
EPSILON = 1e-06
RESIDUAL = 0.25
f32 = jnp.float32
bf16 = jnp.bfloat16
RA = ("z", "y_high", "y_low")
PART = ("z", "y_high")
SUM = ("y_low", "cb")


def exchange(tiles, axis):
    return lax.all_to_all(tiles, axis, 0, 0, tiled=True)


def to_all(tile, axis):
    n = lax.axis_size(axis)
    return exchange(jnp.broadcast_to(tile[None], (n, *tile.shape)), axis)


def coded(part):
    top = jnp.maximum(jnp.max(jnp.abs(part), axis=0, keepdims=True), 1e-30)
    power = jnp.floor(jnp.log2(top))
    return jnp.concatenate([part * jnp.exp2(-power), jnp.broadcast_to(power, (8, part.shape[1]))]).astype(jnp.float16)


def decoded(tiles):
    tiles = tiles.astype(f32)
    width = tiles.shape[1] - 8
    return tiles[:, :width] * jnp.exp2(tiles[:, width : width + 1])


def project(weight, columns):
    return lax.dot_general(weight, columns, (((0,), (0,)), ((), ())), preferred_element_type=f32)


def total(sums):
    return jnp.sum(sums, axis=0, keepdims=True)


def column(row):
    k = row.shape[1]
    same = lax.broadcasted_iota(jnp.int32, (k, k), 0) == lax.broadcasted_iota(jnp.int32, (k, k), 1)
    return jnp.sum(jnp.where(same, row, 0.0), axis=1, keepdims=True)


def stacked(columns):
    high = columns.astype(bf16)
    return jnp.concatenate([high, (columns - high.astype(f32)).astype(bf16)], axis=0)


def rows_of(values):
    at = lax.broadcasted_iota(jnp.int32, (8, values[0].shape[1]), 0)
    rows = jnp.zeros((8, values[0].shape[1]), f32)
    for i, value in enumerate(values):
        rows = jnp.where(at == i, value, rows)
    return rows


def multiply(flat_ref, j, weight, columns):
    twice = jnp.concatenate([weight, weight], axis=0)
    flat_ref[j] = lax.dot_general(twice, columns, (((0,), (0,)), ((), ())), preferred_element_type=f32)


def place(flat_ref, stage_ref, last, owners):
    count, width = flat_ref.shape[:2]
    size = width // stage_ref.shape[0]
    for i in owners:
        for j in range(count):
            stage_ref[i, j * size : (j + 1) * size] = flat_ref[j, i * size : (i + 1) * size]
        stage_ref[i, count * size : count * size + last.shape[0]] = last


def first_kernel(*refs):
    sources, (out_ref, flat_ref, stage_ref, tiles_ref, *held, in_sems, out_sems) = refs[:4], refs[4:]
    pieces = [sources[0], sources[1], sources[2].at[0], sources[3].at[0]]
    copies = [pltpu.make_async_copy(pieces[i], held[i], in_sems.at[i]) for i in range(4)]
    for copy in copies:
        copy.start()
    tokens_ref, pre_ref, gate_ref, up_ref = held
    copies[0].wait()
    copies[1].wait()
    start = tokens_ref[...].astype(f32)
    squares = total(start * start)
    high = squares.astype(bf16).astype(f32)
    sums = rows_of([high, squares - high])[:4]
    columns = stacked(start * column(pre_ref[0:1]))
    for k, ref in enumerate((gate_ref, up_ref)):
        copies[2 + k].wait()
        multiply(flat_ref, k, ref[...], columns)
    n, groups = tiles_ref.shape[0], out_sems.shape[0]
    writes = []
    for g in range(groups):
        part = slice(g * n // groups, (g + 1) * n // groups)
        place(flat_ref, stage_ref, sums, range(part.start, part.stop))
        tiles_ref[part] = stage_ref[part].astype(bf16)
        writes.append(pltpu.make_async_copy(tiles_ref.at[part], out_ref.at[part], out_sems.at[g]))
        writes[-1].start()
    for write in writes:
        write.wait()


def first_tiles(n, *operands):
    width, ntok = operands[-1].shape[2], operands[0].shape[1]
    rows, groups = 2 * (width // n) + 4, 2
    hbm = pl.BlockSpec(memory_space=pltpu.HBM)
    return pl.pallas_call(
        first_kernel,
        out_shape=jax.ShapeDtypeStruct((n, rows, ntok), bf16),
        in_specs=[hbm] * 4,
        out_specs=hbm,
        scratch_shapes=[
            pltpu.VMEM((2, width, ntok), f32),
            pltpu.VMEM((n, rows, ntok), f32),
            pltpu.VMEM((n, rows, ntok), bf16),
            *[pltpu.VMEM(x.shape, x.dtype) for x in operands[:2]],
            *[pltpu.VMEM(x.shape[1:], x.dtype) for x in operands[2:]],
            pltpu.SemaphoreType.DMA((4,)),
            pltpu.SemaphoreType.DMA((groups,)),
        ],
    )(*operands)


def second_kernel(*refs):
    branch_ref, tokens_ref, other_tokens_ref, gains_ref, other_gains_ref, weights_ref, other_weights_ref, *refs = refs
    out_ref, gained_ref, last_ref, flat_ref, stage_ref = refs
    start = jnp.concatenate([tokens_ref[...].astype(f32), other_tokens_ref[...].astype(f32)])
    gains = [jnp.concatenate([column(ref[i : i + 1]) for ref in (gains_ref, other_gains_ref)]) for i in range(3)]
    branch = branch_ref[...]
    gained = branch * gains[1]
    width = gained_ref.shape[0]
    gained_ref[...] = gained[:width]
    last_ref[...] = jnp.broadcast_to(gains[2][:width], gained_ref.shape)
    sums = [total(branch * branch), total(gained * gained), total(start * gained)]
    high = [part.astype(bf16).astype(f32) for part in sums]
    sums = rows_of(high + [part - rounded for part, rounded in zip(sums, high)])
    for i, columns in enumerate((gained, start)):
        columns = stacked(columns * gains[0])
        for k in range(2):
            weight = jnp.concatenate([weights_ref[k], other_weights_ref[k]])
            multiply(flat_ref, 2 * i + k, weight, columns)
    place(flat_ref, stage_ref, sums, range(out_ref.shape[0]))
    out_ref[...] = stage_ref[...].astype(bf16)


def second_tiles(n, *operands):
    (width, ntok), held = operands[1].shape, operands[-1].shape[2]
    rows = 4 * (held // n) + 8
    vmem = pl.BlockSpec(memory_space=pltpu.VMEM)
    return pl.pallas_call(
        second_kernel,
        out_shape=[jax.ShapeDtypeStruct((n, rows, ntok), bf16), *[jax.ShapeDtypeStruct((width, ntok), f32)] * 2],
        in_specs=[vmem] * len(operands),
        out_specs=[vmem] * 3,
        scratch_shapes=[pltpu.VMEM((4, held, ntok), f32), pltpu.VMEM((n, rows, ntok), f32)],
        compiler_params=pltpu.CompilerParams(vmem_limit_bytes=12 * 2**20),
    )(*operands)


def traded(array):
    return lax.ppermute(array, "y_low", [(0, 1), (1, 0)])


def per_device(tokens, pre_gain, post_gain, gate_weight, up_weight, down_weight):
    n = lax.axis_size(RA)
    size = gate_weight.shape[2] // n
    turned = tokens.T
    start = turned.astype(f32)
    width, ntok = start.shape
    low = lax.axis_index("y_low") == 0

    def pair(first, second):
        return jnp.where(low, first, second), jnp.where(low, second, first)

    held = gate_weight.shape[2] // 2
    both = jnp.stack([gate_weight[1], up_weight[1]])
    weights, given = pair(both[:, :, :held], both[:, :, held:])
    down, given_down = pair(down_weight[1, :held], down_weight[1, held:])
    gains = jnp.stack([pre_gain[1], post_gain[0], post_gain[1]])

    tiles = first_tiles(n, turned, pre_gain, gate_weight, up_weight)
    tiles, weights, given, down, given_down, gains = lax.optimization_barrier(
        (tiles, weights, given, down, given_down, gains)
    )
    other_tokens, other_gains, other_weights, other_down = [traded(x) for x in (turned, gains, given, given_down)]
    got = jnp.sum(exchange(tiles, RA).astype(f32), axis=0)
    squares = total(got[2 * size : 2 * size + 2])
    scale_in = lax.rsqrt(squares / D + EPSILON)

    def hidden_of(both, axes):
        hidden = (jax.nn.silu(both[:size]) * both[size:]).astype(bf16)
        return to_all(hidden, axes).reshape(-1, ntok)

    hidden = hidden_of(got[: 2 * size] * scale_in, RA)
    parts = decoded(to_all(coded(project(down_weight[0], hidden)), SUM))
    branch = jnp.concatenate(pair(*jnp.sum(parts.reshape(2, -1, width, ntok), axis=1)))

    tiles, gained, last = second_tiles(
        n // 2, branch, turned, other_tokens, gains, other_gains, weights, other_weights
    )
    got = jnp.sum(exchange(tiles, PART).astype(f32), axis=0)
    sums = got[4 * size : 4 * size + 3] + got[4 * size + 3 : 4 * size + 6]
    branch_sq, gained_sq, cross = sums[0:1], sums[1:2], sums[2:3]
    scale_out = lax.rsqrt(branch_sq / D + EPSILON)
    squares = RESIDUAL * RESIDUAL * squares + 2.0 * RESIDUAL * scale_out * cross + scale_out * scale_out * gained_sq
    scale_in = lax.rsqrt(squares / D + EPSILON)
    stream = RESIDUAL * start + gained * scale_out

    both = (RESIDUAL * got[2 * size : 4 * size] + scale_out * got[: 2 * size]) * scale_in
    hidden = hidden_of(both, PART)
    halves = pair(coded(project(down, hidden)), coded(project(other_down, hidden)))
    members = lax.axis_size("cb")
    parts = jnp.concatenate([jnp.broadcast_to(half[None], (members, *half.shape)) for half in halves])
    branch = jnp.sum(decoded(exchange(parts, SUM)), axis=0)
    branch_sq = jnp.sum(to_all(total(branch * branch), RA), axis=0)
    scale_out = lax.rsqrt(branch_sq / D + EPSILON)
    stream = RESIDUAL * stream + branch * last * scale_out
    return stream.astype(bf16).T


def solution(mesh):
    split = Mesh(mesh.devices.reshape(8, 2, 2, mesh.shape["cb"]), ("z", "y_high", "y_low", "cb"))
    return jax.shard_map(
        per_device,
        mesh=split,
        in_specs=(P(None, RA), P(None, RA), P(None, RA), P(None, RA, "cb"), P(None, RA, "cb"), P(None, "cb", RA)),
        out_specs=P(None, RA),
        check_vma=False,
    )
```

```python
import jax
import jax.numpy as jnp
from jax import lax
from jax.experimental import pallas as pl
from jax.experimental.pallas import tpu as pltpu
from jax.sharding import Mesh
from jax.sharding import PartitionSpec as P


D = 2048
EPSILON = 1e-06
RESIDUAL = 0.25
f32 = jnp.float32
bf16 = jnp.bfloat16
RA = ("z", "y_high", "y_low")
PART = ("z", "y_high")
SUM = ("y_low", "cb")


def exchange(tiles, axis):
    return lax.all_to_all(tiles, axis, 0, 0, tiled=True)


def to_all(tile, axis):
    n = lax.axis_size(axis)
    return exchange(jnp.broadcast_to(tile[None], (n, *tile.shape)), axis)


def coded(part):
    top = jnp.maximum(jnp.max(jnp.abs(part), axis=0, keepdims=True), 1e-30)
    power = jnp.floor(jnp.log2(top))
    return jnp.concatenate([part * jnp.exp2(-power), jnp.broadcast_to(power, (8, part.shape[1]))]).astype(jnp.float16)


def decoded(tiles):
    tiles = tiles.astype(f32)
    width = tiles.shape[1] - 8
    return tiles[:, :width] * jnp.exp2(tiles[:, width : width + 1])


def project(weight, columns):
    return lax.dot_general(weight, columns, (((0,), (0,)), ((), ())), preferred_element_type=f32)


def total(sums):
    return jnp.sum(sums, axis=0, keepdims=True)


def column(row):
    k = row.shape[1]
    same = lax.broadcasted_iota(jnp.int32, (k, k), 0) == lax.broadcasted_iota(jnp.int32, (k, k), 1)
    return jnp.sum(jnp.where(same, row, 0.0), axis=1, keepdims=True)


def stacked(columns):
    high = columns.astype(bf16)
    return jnp.concatenate([high, (columns - high.astype(f32)).astype(bf16)], axis=0)


def rows_of(values):
    at = lax.broadcasted_iota(jnp.int32, (8, values[0].shape[1]), 0)
    rows = jnp.zeros((8, values[0].shape[1]), f32)
    for i, value in enumerate(values):
        rows = jnp.where(at == i, value, rows)
    return rows


def multiply(flat_ref, j, weight, columns):
    twice = jnp.concatenate([weight, weight], axis=0)
    flat_ref[j] = lax.dot_general(twice, columns, (((0,), (0,)), ((), ())), preferred_element_type=f32)


def place(flat_ref, stage_ref, last, owners):
    count, width = flat_ref.shape[:2]
    size = width // stage_ref.shape[0]
    for i in owners:
        for j in range(count):
            stage_ref[i, j * size : (j + 1) * size] = flat_ref[j, i * size : (i + 1) * size]
        stage_ref[i, count * size : count * size + last.shape[0]] = last


def gain_lanes(gains):
    lane = lax.broadcasted_iota(jnp.int32, (gains[0].shape[0], 128), 1)
    lanes = jnp.zeros(lane.shape, f32)
    for i, rest in enumerate(gains):
        for k in range(3):
            part = rest.astype(bf16).astype(f32)
            lanes = jnp.where(lane == 3 * i + k, part, lanes)
            rest = rest - part
    return lanes.astype(bf16)


def gain_of(lanes, i):
    lane = lax.broadcasted_iota(jnp.int32, lanes.shape, 1)
    return jnp.sum(jnp.where(lane // 3 == i, lanes.astype(f32), 0.0), axis=1, keepdims=True)


def first_kernel(*refs):
    sources, (out_ref, side_out_ref, flat_ref, stage_ref, tiles_ref, side_ref, *held, in_sems, out_sems) = refs[:5], refs[5:]
    pieces = [*sources[:3], sources[3].at[0], sources[4].at[0]]
    copies = [pltpu.make_async_copy(pieces[i], held[i], in_sems.at[i]) for i in range(5)]
    for copy in copies:
        copy.start()
    tokens_ref, pre_ref, post_ref, gate_ref, up_ref = held
    for copy in copies[:3]:
        copy.wait()
    ntok = tokens_ref.shape[1]
    side_ref[:, :ntok] = tokens_ref[...]
    side_ref[:, ntok:] = gain_lanes([column(row) for row in (pre_ref[1:2], post_ref[0:1], post_ref[1:2])])
    groups = out_sems.shape[0] - 1
    writes = [pltpu.make_async_copy(side_ref, side_out_ref, out_sems.at[groups])]
    writes[0].start()
    start = tokens_ref[...].astype(f32)
    squares = total(start * start)
    high = squares.astype(bf16).astype(f32)
    sums = rows_of([high, squares - high])[:4]
    columns = stacked(start * column(pre_ref[0:1]))
    for k, ref in enumerate((gate_ref, up_ref)):
        copies[3 + k].wait()
        multiply(flat_ref, k, ref[...], columns)
    n = tiles_ref.shape[0]
    for g in range(groups):
        part = slice(g * n // groups, (g + 1) * n // groups)
        place(flat_ref, stage_ref, sums, range(part.start, part.stop))
        tiles_ref[part] = stage_ref[part].astype(bf16)
        writes.append(pltpu.make_async_copy(tiles_ref.at[part], out_ref.at[part], out_sems.at[g]))
        writes[-1].start()
    for write in writes:
        write.wait()


def first_tiles(n, *operands):
    width, ntok = operands[-1].shape[2], operands[0].shape[1]
    rows, groups = 2 * (width // n) + 4, 2
    side = operands[0].shape[0], ntok + 128
    hbm = pl.BlockSpec(memory_space=pltpu.HBM)
    return pl.pallas_call(
        first_kernel,
        out_shape=[jax.ShapeDtypeStruct((n, rows, ntok), bf16), jax.ShapeDtypeStruct(side, bf16)],
        in_specs=[hbm] * 5,
        out_specs=[hbm] * 2,
        scratch_shapes=[
            pltpu.VMEM((2, width, ntok), f32),
            pltpu.VMEM((n, rows, ntok), f32),
            pltpu.VMEM((n, rows, ntok), bf16),
            pltpu.VMEM(side, bf16),
            *[pltpu.VMEM(x.shape, x.dtype) for x in operands[:3]],
            *[pltpu.VMEM(x.shape[1:], x.dtype) for x in operands[3:]],
            pltpu.SemaphoreType.DMA((5,)),
            pltpu.SemaphoreType.DMA((groups + 1,)),
        ],
    )(*operands)


def second_kernel(*refs):
    branch_ref, side_ref, other_ref, weights_ref, out_ref, gained_ref, last_ref, flat_ref, stage_ref = refs
    width, ntok = gained_ref.shape
    held = weights_ref.shape[2]
    other = other_ref.shape[1] - side_ref.shape[1]
    start = jnp.concatenate([side_ref[:, :ntok], other_ref[:, other : other + ntok]]).astype(f32)
    lanes = side_ref[:, ntok:], other_ref[:, other + ntok :]
    gains = [jnp.concatenate([gain_of(part, i) for part in lanes]) for i in range(3)]
    branch = branch_ref[...]
    gained = branch * gains[1]
    gained_ref[...] = gained[:width]
    last_ref[...] = jnp.broadcast_to(gains[2][:width], gained_ref.shape)
    sums = [total(branch * branch), total(gained * gained), total(start * gained)]
    high = [part.astype(bf16).astype(f32) for part in sums]
    sums = rows_of(high + [part - rounded for part, rounded in zip(sums, high)])
    for i, columns in enumerate((gained, start)):
        columns = stacked(columns * gains[0])
        for k in range(2):
            weight = jnp.concatenate([weights_ref[k], other_ref[:, k * other // 2 : k * other // 2 + held]])
            multiply(flat_ref, 2 * i + k, weight, columns)
    place(flat_ref, stage_ref, sums, range(out_ref.shape[0]))
    out_ref[...] = stage_ref[...].astype(bf16)


def second_tiles(n, *operands):
    (width, ntok), held = (operands[1].shape[0], operands[0].shape[1]), operands[-1].shape[2]
    rows = 4 * (held // n) + 8
    vmem = pl.BlockSpec(memory_space=pltpu.VMEM)
    return pl.pallas_call(
        second_kernel,
        out_shape=[jax.ShapeDtypeStruct((n, rows, ntok), bf16), *[jax.ShapeDtypeStruct((width, ntok), f32)] * 2],
        in_specs=[vmem] * len(operands),
        out_specs=[vmem] * 3,
        scratch_shapes=[pltpu.VMEM((4, held, ntok), f32), pltpu.VMEM((n, rows, ntok), f32)],
        compiler_params=pltpu.CompilerParams(vmem_limit_bytes=12 * 2**20),
    )(*operands)


def traded(array):
    return lax.ppermute(array, "y_low", [(0, 1), (1, 0)])


def sublayers(tokens, pre_gain, post_gain, gate_weight, up_weight, down_weight):
    n = lax.axis_size(RA)
    size = gate_weight.shape[2] // n
    turned = tokens.T
    start = turned.astype(f32)
    width, ntok = start.shape
    low = lax.axis_index("y_low") == 0

    def pair(first, second):
        return jnp.where(low, first, second), jnp.where(low, second, first)

    tiles, side = first_tiles(n, turned, pre_gain, post_gain, gate_weight, up_weight)

    held = gate_weight.shape[2] // 2
    weights, given = zip(*[pair(weight[1, :, :held], weight[1, :, held:]) for weight in (gate_weight, up_weight)])
    down, given_down = pair(down_weight[1, :held], down_weight[1, held:])
    given = jnp.concatenate([*[jnp.pad(part, ((0, 0), (0, -held % 128))) for part in given], side], axis=1)
    tiles, weights, given, down, given_down = lax.optimization_barrier(
        (tiles, jnp.stack(weights), given, down, given_down)
    )
    other = traded(given)
    other_down = traded(given_down)
    got = exchange(tiles, RA)
    got = jnp.sum(got.astype(f32), axis=0)
    squares = total(got[2 * size : 2 * size + 2])
    scale_in = lax.rsqrt(squares / D + EPSILON)

    def hidden_of(both, axes):
        hidden = (jax.nn.silu(both[:size]) * both[size:]).astype(bf16)
        return to_all(hidden, axes).reshape(-1, ntok)

    hidden = hidden_of(got[: 2 * size] * scale_in, RA)
    parts = decoded(to_all(coded(project(down_weight[0], hidden)), SUM))
    branch = jnp.concatenate(pair(*jnp.sum(parts.reshape(2, -1, width, ntok), axis=1)))

    tiles, gained, last = second_tiles(n // 2, branch, side, other, weights)
    got = jnp.sum(exchange(tiles, PART).astype(f32), axis=0)
    sums = got[4 * size : 4 * size + 3] + got[4 * size + 3 : 4 * size + 6]
    branch_sq, gained_sq, cross = sums[0:1], sums[1:2], sums[2:3]
    scale_out = lax.rsqrt(branch_sq / D + EPSILON)
    squares = RESIDUAL * RESIDUAL * squares + 2.0 * RESIDUAL * scale_out * cross + scale_out * scale_out * gained_sq
    scale_in = lax.rsqrt(squares / D + EPSILON)
    stream = RESIDUAL * start + gained * scale_out

    both = (RESIDUAL * got[2 * size : 4 * size] + scale_out * got[: 2 * size]) * scale_in
    hidden = hidden_of(both, PART)
    halves = pair(coded(project(down, hidden)), coded(project(other_down, hidden)))
    members = lax.axis_size("cb")
    parts = jnp.concatenate([jnp.broadcast_to(half[None], (members, *half.shape)) for half in halves])
    branch = jnp.sum(decoded(exchange(parts, SUM)), axis=0)
    branch_sq = jnp.sum(to_all(total(branch * branch), RA), axis=0)
    scale_out = lax.rsqrt(branch_sq / D + EPSILON)
    stream = RESIDUAL * stream + branch * last * scale_out
    return stream.astype(bf16).T


def solution(mesh):
    split = Mesh(mesh.devices.reshape(8, 2, 2, mesh.shape["cb"]), ("z", "y_high", "y_low", "cb"))
    return jax.shard_map(
        sublayers,
        mesh=split,
        in_specs=(P(None, RA), P(None, RA), P(None, RA), P(None, RA, "cb"), P(None, RA, "cb"), P(None, "cb", RA)),
        out_specs=P(None, RA),
        check_vma=False,
    )
```

```python
import jax
import jax.numpy as jnp
from jax import lax
from jax.experimental import pallas as pl
from jax.experimental.pallas import tpu as pltpu
from jax.sharding import Mesh
from jax.sharding import PartitionSpec as P


D = 2048
EPSILON = 1e-06
RESIDUAL = 0.25
f32 = jnp.float32
bf16 = jnp.bfloat16
RA = ("z", "y_high", "y_low")
PART = ("z", "y_high")
SUM = ("y_low", "cb")


def exchange(tiles, axis):
    return lax.all_to_all(tiles, axis, 0, 0, tiled=True)


def to_all(tile, axis):
    n = lax.axis_size(axis)
    return exchange(jnp.broadcast_to(tile[None], (n, *tile.shape)), axis)


def coded(part):
    top = jnp.maximum(jnp.max(jnp.abs(part), axis=0, keepdims=True), 1e-30)
    power = jnp.floor(jnp.log2(top))
    return jnp.concatenate([part * jnp.exp2(-power), jnp.broadcast_to(power, (8, part.shape[1]))]).astype(jnp.float16)


def decoded(tiles):
    tiles = tiles.astype(f32)
    width = tiles.shape[1] - 8
    return tiles[:, :width] * jnp.exp2(tiles[:, width : width + 1])


def down_project(weight, columns):
    return jnp.dot(weight, columns, preferred_element_type=f32)


def total(sums):
    return jnp.sum(sums, axis=0, keepdims=True)


def column(row):
    k = row.shape[1]
    same = lax.broadcasted_iota(jnp.int32, (k, k), 0) == lax.broadcasted_iota(jnp.int32, (k, k), 1)
    return jnp.sum(jnp.where(same, row, 0.0), axis=1, keepdims=True)


def stacked(columns):
    high = columns.astype(bf16)
    return jnp.concatenate([high, (columns - high.astype(f32)).astype(bf16)], axis=0)


def rows_of(values):
    at = lax.broadcasted_iota(jnp.int32, (8, values[0].shape[1]), 0)
    rows = jnp.zeros((8, values[0].shape[1]), f32)
    for i, value in enumerate(values):
        rows = jnp.where(at == i, value, rows)
    return rows


def multiply(flat_ref, j, weight, columns):
    twice = jnp.concatenate([weight, weight], axis=0)
    flat_ref[j] = lax.dot_general(twice, columns, (((0,), (0,)), ((), ())), preferred_element_type=f32)


def place(flat_ref, stage_ref, last, owners):
    count, width = flat_ref.shape[:2]
    size = width // stage_ref.shape[0]
    for i in owners:
        for j in range(count):
            stage_ref[i, j * size : (j + 1) * size] = flat_ref[j, i * size : (i + 1) * size]
        stage_ref[i, count * size : count * size + last.shape[0]] = last


def gain_lanes(gains):
    lane = lax.broadcasted_iota(jnp.int32, (gains[0].shape[0], 128), 1)
    lanes = jnp.zeros(lane.shape, f32)
    for i, rest in enumerate(gains):
        for k in range(3):
            part = rest.astype(bf16).astype(f32)
            lanes = jnp.where(lane == 3 * i + k, part, lanes)
            rest = rest - part
    return lanes.astype(bf16)


def gain_of(lanes, i):
    lane = lax.broadcasted_iota(jnp.int32, lanes.shape, 1)
    return jnp.sum(jnp.where(lane // 3 == i, lanes.astype(f32), 0.0), axis=1, keepdims=True)


def first_kernel(*refs):
    sources, (out_ref, keep_out_ref, give_out_ref, *refs) = refs[:6], refs[6:]
    flat_ref, stage_ref, tiles_ref, keep_ref, give_ref, turn_ref, *held, in_sems, out_sems = refs
    pieces = [*sources[:3], sources[3].at[0], sources[4].at[0], *[source.at[1] for source in sources[3:]]]
    copies = [pltpu.make_async_copy(pieces[i], held[i], in_sems.at[i]) for i in range(8)]
    for copy in copies:
        copy.start()
    tokens_ref, pre_ref, post_ref, gate_ref, up_ref, *traded_refs = held
    for copy in copies[:3]:
        copy.wait()
    start = tokens_ref[...].astype(f32)
    squares = total(start * start)
    high = squares.astype(bf16).astype(f32)
    sums = rows_of([high, squares - high])[:4]
    columns = stacked(start * column(pre_ref[0:1]))
    for k, ref in enumerate((gate_ref, up_ref)):
        copies[3 + k].wait()
        multiply(flat_ref, k, ref[...], columns)
    n, groups = tiles_ref.shape[0], out_sems.shape[0] - 2
    writes = []
    for g in range(groups):
        part = slice(g * n // groups, (g + 1) * n // groups)
        place(flat_ref, stage_ref, sums, range(part.start, part.stop))
        tiles_ref[part] = stage_ref[part].astype(bf16)
        writes.append(pltpu.make_async_copy(tiles_ref.at[part], out_ref.at[part], out_sems.at[g]))
        writes[-1].start()

    low = lax.axis_index("y_low") == 0
    width, wide = traded_refs[0].shape[1], turn_ref.shape[1]
    half, step = width // 2, wide // 2
    for k, ref in enumerate(traded_refs):
        copies[5 + k].wait()
        turn_ref[:, :width] = ref[...].astype(f32)
        first, second = turn_ref[:, :half], pltpu.roll(turn_ref[...], wide - half, 1)[:, :half]
        keep_ref[:, k * step : k * step + half] = jnp.where(low, first, second).astype(bf16)
        give_ref[:, k * step : k * step + half] = jnp.where(low, second, first).astype(bf16)
    ntok = tokens_ref.shape[1]
    gains = gain_lanes([column(row) for row in (pre_ref[1:2], post_ref[0:1], post_ref[1:2])])
    for ref in (keep_ref, give_ref):
        ref[:, 3 * step : 3 * step + ntok] = tokens_ref[...]
        ref[:, 3 * step + ntok :] = gains
    for i, (source, target) in enumerate(((keep_ref, keep_out_ref), (give_ref, give_out_ref))):
        writes.append(pltpu.make_async_copy(source, target, out_sems.at[groups + i]))
        writes[-1].start()
    for write in writes:
        write.wait()


def first_tiles(n, *operands):
    (count, ntok), width = operands[0].shape, operands[-1].shape[2]
    rows, groups, step = 2 * (width // n) + 4, 2, -(-width // 256) * 128
    outs = [jax.ShapeDtypeStruct(shape, bf16) for shape in ((n, rows, ntok), *[(count, 3 * step + ntok + 128)] * 2)]
    hbm = pl.BlockSpec(memory_space=pltpu.HBM)
    return pl.pallas_call(
        first_kernel,
        out_shape=outs,
        in_specs=[hbm] * 6,
        out_specs=[hbm] * 3,
        scratch_shapes=[
            pltpu.VMEM((2, width, ntok), f32),
            pltpu.VMEM((n, rows, ntok), f32),
            *[pltpu.VMEM(out.shape, bf16) for out in outs],
            pltpu.VMEM((count, 2 * step), f32),
            *[pltpu.VMEM(x.shape, x.dtype) for x in operands[:3]],
            *[pltpu.VMEM((count, width), bf16) for _ in range(5)],
            pltpu.SemaphoreType.DMA((8,)),
            pltpu.SemaphoreType.DMA((groups + 2,)),
        ],
    )(*operands)


def second_kernel(*refs):
    branch_ref, mine_ref, other_ref, out_ref, start_ref, gained_ref, last_ref, flat_ref, stage_ref = refs
    width, ntok = gained_ref.shape
    held, step = flat_ref.shape[1], (mine_ref.shape[1] - ntok - 128) // 3
    sides = [ref[:, 3 * step :] for ref in (mine_ref, other_ref)]
    start = jnp.concatenate([side[:, :ntok] for side in sides]).astype(f32)
    start_ref[...] = start[:width]
    gains = [jnp.concatenate([gain_of(side[:, ntok:], i) for side in sides]) for i in range(3)]
    branch = branch_ref[...]
    gained = branch * gains[1]
    gained_ref[...] = gained[:width]
    last_ref[...] = jnp.broadcast_to(gains[2][:width], gained_ref.shape)
    sums = [total(branch * branch), total(gained * gained), total(start * gained)]
    high = [part.astype(bf16).astype(f32) for part in sums]
    sums = rows_of(high + [part - rounded for part, rounded in zip(sums, high)])
    for i, columns in enumerate((gained, start)):
        columns = stacked(columns * gains[0])
        for k in range(2):
            weight = jnp.concatenate([ref[:, k * step : k * step + held] for ref in (mine_ref, other_ref)])
            multiply(flat_ref, 2 * i + k, weight, columns)
    place(flat_ref, stage_ref, sums, range(out_ref.shape[0]))
    out_ref[...] = stage_ref[...].astype(bf16)


def second_tiles(n, held, *operands):
    width, ntok = operands[1].shape[0], operands[0].shape[1]
    rows = 4 * (held // n) + 8
    vmem = pl.BlockSpec(memory_space=pltpu.VMEM)
    return pl.pallas_call(
        second_kernel,
        out_shape=[jax.ShapeDtypeStruct((n, rows, ntok), bf16), *[jax.ShapeDtypeStruct((width, ntok), f32)] * 3],
        in_specs=[vmem] * len(operands),
        out_specs=[vmem] * 4,
        scratch_shapes=[pltpu.VMEM((4, held, ntok), f32), pltpu.VMEM((n, rows, ntok), f32)],
        compiler_params=pltpu.CompilerParams(vmem_limit_bytes=12 * 2**20),
    )(*operands)


def traded(array):
    return lax.ppermute(array, "y_low", [(0, 1), (1, 0)])


def sublayers(tokens, pre_gain, post_gain, gate_weight, up_weight, down_weight):
    n = lax.axis_size(RA)
    size = gate_weight.shape[2] // n
    turned = tokens.T
    width, ntok = turned.shape
    low = lax.axis_index("y_low") == 0

    def pair(first, second):
        return jnp.where(low, first, second), jnp.where(low, second, first)

    held = gate_weight.shape[2] // 2
    down_weight = down_weight.transpose(0, 2, 1)
    tiles, keep, give = first_tiles(n, turned, pre_gain, post_gain, gate_weight, up_weight, down_weight)
    tiles, low = lax.optimization_barrier((tiles, low))
    other = traded(give)
    got = exchange(tiles, RA)
    got = jnp.sum(got.astype(f32), axis=0)
    squares = total(got[2 * size : 2 * size + 2])
    scale_in = lax.rsqrt(squares / D + EPSILON)

    def hidden_of(both, axes):
        hidden = (jax.nn.silu(both[:size]) * both[size:]).astype(bf16)
        return to_all(hidden, axes).reshape(-1, ntok)

    hidden = hidden_of(got[: 2 * size] * scale_in, RA)
    parts = decoded(to_all(coded(down_project(down_weight[0], hidden)), SUM))
    branch = jnp.concatenate(pair(*jnp.sum(parts.reshape(2, -1, width, ntok), axis=1)))

    tiles, start, gained, last = second_tiles(n // 2, held, branch, keep, other)
    got = jnp.sum(exchange(tiles, PART).astype(f32), axis=0)
    sums = got[4 * size : 4 * size + 3] + got[4 * size + 3 : 4 * size + 6]
    branch_sq, gained_sq, cross = sums[0:1], sums[1:2], sums[2:3]
    scale_out = lax.rsqrt(branch_sq / D + EPSILON)
    squares = RESIDUAL * RESIDUAL * squares + 2.0 * RESIDUAL * scale_out * cross + scale_out * scale_out * gained_sq
    scale_in = lax.rsqrt(squares / D + EPSILON)
    stream = RESIDUAL * start + gained * scale_out

    both = (RESIDUAL * got[2 * size : 4 * size] + scale_out * got[: 2 * size]) * scale_in
    hidden = hidden_of(both, PART)
    step = -(-held // 128) * 128
    halves = pair(*[coded(down_project(x[:, 2 * step : 2 * step + held], hidden)) for x in (keep, other)])
    members = lax.axis_size("cb")
    parts = jnp.concatenate([jnp.broadcast_to(half[None], (members, *half.shape)) for half in halves])
    branch = jnp.sum(decoded(exchange(parts, SUM)), axis=0)
    branch_sq = jnp.sum(to_all(total(branch * branch), RA), axis=0)
    scale_out = lax.rsqrt(branch_sq / D + EPSILON)
    stream = RESIDUAL * stream + branch * last * scale_out
    return stream.astype(bf16).T


def solution(mesh):
    split = Mesh(mesh.devices.reshape(8, 2, 2, mesh.shape["cb"]), ("z", "y_high", "y_low", "cb"))
    return jax.shard_map(
        sublayers,
        mesh=split,
        in_specs=(P(None, RA), P(None, RA), P(None, RA), P(None, RA, "cb"), P(None, RA, "cb"), P(None, "cb", RA)),
        out_specs=P(None, RA),
        check_vma=False,
    )
```

```python
import jax
import jax.numpy as jnp
from jax import lax
from jax.experimental import pallas as pl
from jax.experimental.pallas import tpu as pltpu
from jax.sharding import Mesh
from jax.sharding import PartitionSpec as P


D = 2048
EPSILON = 1e-06
RESIDUAL = 0.25
f32 = jnp.float32
bf16 = jnp.bfloat16
RA = ("z", "y_high", "y_low")
PART = ("z", "y_high")
SUM = ("y_low", "cb")


def exchange(tiles, axis):
    return lax.all_to_all(tiles, axis, 0, 0, tiled=True)


def to_all(tile, axis):
    n = lax.axis_size(axis)
    return exchange(jnp.broadcast_to(tile[None], (n, *tile.shape)), axis)


def coded(part):
    top = jnp.maximum(jnp.max(jnp.abs(part), axis=0, keepdims=True), 1e-30)
    power = jnp.floor(jnp.log2(top))
    return jnp.concatenate([part * jnp.exp2(-power), jnp.broadcast_to(power, (8, part.shape[1]))]).astype(jnp.float16)


def decoded(tiles):
    tiles = tiles.astype(f32)
    width = tiles.shape[1] - 8
    return tiles[:, :width] * jnp.exp2(tiles[:, width : width + 1])


def down_project(weight, columns):
    return jnp.dot(weight, columns, preferred_element_type=f32)


def total(sums):
    return jnp.sum(sums, axis=0, keepdims=True)


def column(row):
    k = row.shape[1]
    same = lax.broadcasted_iota(jnp.int32, (k, k), 0) == lax.broadcasted_iota(jnp.int32, (k, k), 1)
    return jnp.sum(jnp.where(same, row, 0.0), axis=1, keepdims=True)


def stacked(columns):
    high = columns.astype(bf16)
    return jnp.concatenate([high, (columns - high.astype(f32)).astype(bf16)], axis=0)


def rows_of(values):
    at = lax.broadcasted_iota(jnp.int32, (8, values[0].shape[1]), 0)
    rows = jnp.zeros((8, values[0].shape[1]), f32)
    for i, value in enumerate(values):
        rows = jnp.where(at == i, value, rows)
    return rows


def multiply(flat_ref, j, weight, columns):
    twice = jnp.concatenate([weight, weight], axis=0)
    flat_ref[j] = lax.dot_general(twice, columns, (((0,), (0,)), ((), ())), preferred_element_type=f32)


def place(flat_ref, stage_ref, last, owners):
    count, width = flat_ref.shape[:2]
    size = width // stage_ref.shape[0]
    for i in owners:
        for j in range(count):
            stage_ref[i, j * size : (j + 1) * size] = flat_ref[j, i * size : (i + 1) * size]
        stage_ref[i, count * size : count * size + last.shape[0]] = last


def gain_lanes(gains):
    lane = lax.broadcasted_iota(jnp.int32, (gains[0].shape[0], 128), 1)
    lanes = jnp.zeros(lane.shape, f32)
    for i, rest in enumerate(gains):
        for k in range(3):
            part = rest.astype(bf16).astype(f32)
            lanes = jnp.where(lane == 3 * i + k, part, lanes)
            rest = rest - part
    return lanes.astype(bf16)


def gain_of(lanes, i):
    lane = lax.broadcasted_iota(jnp.int32, lanes.shape, 1)
    return jnp.sum(jnp.where(lane // 3 == i, lanes.astype(f32), 0.0), axis=1, keepdims=True)


def first_kernel(*refs):
    sources, (out_ref, keep_out_ref, give_out_ref, *refs) = refs[:6], refs[6:]
    flat_ref, stage_ref, tiles_ref, keep_ref, give_ref, turn_ref, *held, in_sems, out_sems = refs
    pieces = [*sources[:3], sources[3].at[0], sources[4].at[0], *[source.at[1] for source in sources[3:]]]
    copies = [pltpu.make_async_copy(pieces[i], held[i], in_sems.at[i]) for i in range(8)]
    for copy in copies:
        copy.start()
    tokens_ref, pre_ref, post_ref, gate_ref, up_ref, *traded_refs = held
    for copy in copies[:3]:
        copy.wait()
    start = tokens_ref[...].astype(f32)
    squares = total(start * start)
    high = squares.astype(bf16).astype(f32)
    sums = rows_of([high, squares - high])[:4]
    columns = stacked(start * column(pre_ref[0:1]))
    for k, ref in enumerate((gate_ref, up_ref)):
        copies[3 + k].wait()
        multiply(flat_ref, k, ref[...], columns)
    n, groups = tiles_ref.shape[0], out_sems.shape[0] - 2
    writes = []
    for g in range(groups):
        part = slice(g * n // groups, (g + 1) * n // groups)
        place(flat_ref, stage_ref, sums, range(part.start, part.stop))
        tiles_ref[part] = stage_ref[part].astype(bf16)
        writes.append(pltpu.make_async_copy(tiles_ref.at[part], out_ref.at[part], out_sems.at[g]))
        writes[-1].start()

    low = lax.axis_index("y_low") == 0
    width, wide = traded_refs[0].shape[1], turn_ref.shape[1]
    half, step = width // 2, wide // 2
    for k, ref in enumerate(traded_refs):
        copies[5 + k].wait()
        turn_ref[:, :width] = ref[...].astype(f32)
        first, second = turn_ref[:, :half], pltpu.roll(turn_ref[...], wide - half, 1)[:, :half]
        keep_ref[:, k * step : k * step + half] = jnp.where(low, first, second).astype(bf16)
        give_ref[:, k * step : k * step + half] = jnp.where(low, second, first).astype(bf16)
    ntok = tokens_ref.shape[1]
    gains = gain_lanes([column(row) for row in (pre_ref[1:2], post_ref[0:1], post_ref[1:2])])
    for ref in (keep_ref, give_ref):
        ref[:, 3 * step : 3 * step + ntok] = tokens_ref[...]
        ref[:, 3 * step + ntok :] = gains
    for i, (source, target) in enumerate(((keep_ref, keep_out_ref), (give_ref, give_out_ref))):
        writes.append(pltpu.make_async_copy(source, target, out_sems.at[groups + i]))
        writes[-1].start()
    for write in writes:
        write.wait()


def first_tiles(n, *operands):
    (count, ntok), width = operands[0].shape, operands[-1].shape[2]
    rows, groups, step = 2 * (width // n) + 4, 2, -(-width // 256) * 128
    outs = [jax.ShapeDtypeStruct(shape, bf16) for shape in ((n, rows, ntok), *[(count, 3 * step + ntok + 128)] * 2)]
    hbm = pl.BlockSpec(memory_space=pltpu.HBM)
    return pl.pallas_call(
        first_kernel,
        out_shape=outs,
        in_specs=[hbm] * 6,
        out_specs=[hbm] * 3,
        scratch_shapes=[
            pltpu.VMEM((2, width, ntok), f32),
            pltpu.VMEM((n, rows, ntok), f32),
            *[pltpu.VMEM(out.shape, bf16) for out in outs],
            pltpu.VMEM((count, 2 * step), f32),
            *[pltpu.VMEM(x.shape, x.dtype) for x in operands[:3]],
            *[pltpu.VMEM((count, width), bf16) for _ in range(5)],
            pltpu.SemaphoreType.DMA((8,)),
            pltpu.SemaphoreType.DMA((groups + 2,)),
        ],
    )(*operands)


def second_kernel(*refs):
    branch_ref, mine_ref, side_ref, other_ref, out_ref, start_ref, gained_ref, last_ref, flat_ref, stage_ref = refs
    width, ntok = gained_ref.shape
    held, step = flat_ref.shape[1], mine_ref.shape[1] // 3
    sides = side_ref[...], other_ref[:, 3 * step :]
    start = jnp.concatenate([side[:, :ntok] for side in sides]).astype(f32)
    start_ref[...] = start[:width]
    gains = [jnp.concatenate([gain_of(side[:, ntok:], i) for side in sides]) for i in range(3)]
    branch = branch_ref[...]
    gained = branch * gains[1]
    gained_ref[...] = gained[:width]
    last_ref[...] = jnp.broadcast_to(gains[2][:width], gained_ref.shape)
    sums = [total(branch * branch), total(gained * gained), total(start * gained)]
    high = [part.astype(bf16).astype(f32) for part in sums]
    sums = rows_of(high + [part - rounded for part, rounded in zip(sums, high)])
    for i, columns in enumerate((gained, start)):
        columns = stacked(columns * gains[0])
        for k in range(2):
            weight = jnp.concatenate([ref[:, k * step : k * step + held] for ref in (mine_ref, other_ref)])
            multiply(flat_ref, 2 * i + k, weight, columns)
    place(flat_ref, stage_ref, sums, range(out_ref.shape[0]))
    out_ref[...] = stage_ref[...].astype(bf16)


def second_tiles(n, held, *operands):
    width, ntok = operands[1].shape[0], operands[0].shape[1]
    rows = 4 * (held // n) + 8
    vmem = pl.BlockSpec(memory_space=pltpu.VMEM)
    return pl.pallas_call(
        second_kernel,
        out_shape=[jax.ShapeDtypeStruct((n, rows, ntok), bf16), *[jax.ShapeDtypeStruct((width, ntok), f32)] * 3],
        in_specs=[vmem] * len(operands),
        out_specs=[vmem] * 4,
        scratch_shapes=[pltpu.VMEM((4, held, ntok), f32), pltpu.VMEM((n, rows, ntok), f32)],
        compiler_params=pltpu.CompilerParams(vmem_limit_bytes=12 * 2**20),
    )(*operands)


def traded(array):
    return lax.ppermute(array, "y_low", [(0, 1), (1, 0)])


def sublayers(tokens, pre_gain, post_gain, gate_weight, up_weight, down_weight):
    n = lax.axis_size(RA)
    size = gate_weight.shape[2] // n
    turned = tokens.T
    width, ntok = turned.shape
    low = lax.axis_index("y_low") == 0

    def pair(first, second):
        return jnp.where(low, first, second), jnp.where(low, second, first)

    held = gate_weight.shape[2] // 2
    down_weight = down_weight.transpose(0, 2, 1)
    tiles, keep, give = first_tiles(n, turned, pre_gain, post_gain, gate_weight, up_weight, down_weight)
    down_now = jnp.where(low, down_weight[0], down_weight[0] * 1)
    tiles, low, down_now = lax.optimization_barrier((tiles, low, down_now))
    other = traded(give)
    got = exchange(tiles, RA)
    step = -(-held // 128) * 128
    got, keep, side = lax.optimization_barrier((got, keep[:, : 3 * step], keep[:, 3 * step :]))
    got = jnp.sum(got.astype(f32), axis=0)
    squares = total(got[2 * size : 2 * size + 2])
    scale_in = lax.rsqrt(squares / D + EPSILON)

    def hidden_of(both, axes):
        hidden = (jax.nn.silu(both[:size]) * both[size:]).astype(bf16)
        return to_all(hidden, axes).reshape(-1, ntok)

    hidden = hidden_of(got[: 2 * size] * scale_in, RA)
    parts = decoded(to_all(coded(down_project(down_now, hidden)), SUM))
    branch = jnp.concatenate(pair(*jnp.sum(parts.reshape(2, -1, width, ntok), axis=1)))

    tiles, start, gained, last = second_tiles(n // 2, held, branch, keep, side, other)
    got = jnp.sum(exchange(tiles, PART).astype(f32), axis=0)
    sums = got[4 * size : 4 * size + 3] + got[4 * size + 3 : 4 * size + 6]
    branch_sq, gained_sq, cross = sums[0:1], sums[1:2], sums[2:3]
    scale_out = lax.rsqrt(branch_sq / D + EPSILON)
    squares = RESIDUAL * RESIDUAL * squares + 2.0 * RESIDUAL * scale_out * cross + scale_out * scale_out * gained_sq
    scale_in = lax.rsqrt(squares / D + EPSILON)
    stream = RESIDUAL * start + gained * scale_out

    both = (RESIDUAL * got[2 * size : 4 * size] + scale_out * got[: 2 * size]) * scale_in
    hidden = hidden_of(both, PART)
    halves = pair(*[coded(down_project(x[:, 2 * step : 2 * step + held], hidden)) for x in (keep, other)])
    members = lax.axis_size("cb")
    parts = jnp.concatenate([jnp.broadcast_to(half[None], (members, *half.shape)) for half in halves])
    branch = jnp.sum(decoded(exchange(parts, SUM)), axis=0)
    branch_sq = jnp.sum(to_all(total(branch * branch), RA), axis=0)
    scale_out = lax.rsqrt(branch_sq / D + EPSILON)
    stream = RESIDUAL * stream + branch * last * scale_out
    return stream.astype(bf16).T


def solution(mesh):
    split = Mesh(mesh.devices.reshape(8, 2, 2, mesh.shape["cb"]), ("z", "y_high", "y_low", "cb"))
    return jax.shard_map(
        sublayers,
        mesh=split,
        in_specs=(P(None, RA), P(None, RA), P(None, RA), P(None, RA, "cb"), P(None, RA, "cb"), P(None, "cb", RA)),
        out_specs=P(None, RA),
        check_vma=False,
    )
```

```python
import jax
import jax.numpy as jnp
from jax import lax
from jax.experimental import pallas as pl
from jax.experimental.pallas import tpu as pltpu
from jax.sharding import Mesh
from jax.sharding import PartitionSpec as P


D = 2048
EPSILON = 1e-06
RESIDUAL = 0.25
f32 = jnp.float32
bf16 = jnp.bfloat16
RA = ("z", "y_high", "y_low")
PARTS = [[4 * z + y for z in range(8) for y in ys] for ys in ((0, 3), (1, 2))]
SUM = ("y_low", "cb")


def exchange(tiles, axis, groups=None):
    return lax.all_to_all(tiles, axis, 0, 0, axis_index_groups=groups, tiled=True)


def to_all(tile, axis, groups=None):
    n = len(groups[0]) if groups else lax.axis_size(axis)
    return exchange(jnp.broadcast_to(tile[None], (n, *tile.shape)), axis, groups)


def coded(part):
    top = jnp.maximum(jnp.max(jnp.abs(part), axis=0, keepdims=True), 1e-30)
    power = jnp.floor(jnp.log2(top))
    return jnp.concatenate([part * jnp.exp2(-power), jnp.broadcast_to(power, (8, part.shape[1]))]).astype(jnp.float16)


def decoded(tiles):
    tiles = tiles.astype(f32)
    width = tiles.shape[1] - 8
    return tiles[:, :width] * jnp.exp2(tiles[:, width : width + 1])


def down_project(weight, columns):
    return jnp.dot(weight, columns, preferred_element_type=f32)


def total(sums):
    return jnp.sum(sums, axis=0, keepdims=True)


def column(row):
    k = row.shape[1]
    same = lax.broadcasted_iota(jnp.int32, (k, k), 0) == lax.broadcasted_iota(jnp.int32, (k, k), 1)
    return jnp.sum(jnp.where(same, row, 0.0), axis=1, keepdims=True)


def stacked(columns):
    high = columns.astype(bf16)
    return jnp.concatenate([high, (columns - high.astype(f32)).astype(bf16)], axis=0)


def rows_of(values):
    at = lax.broadcasted_iota(jnp.int32, (8, values[0].shape[1]), 0)
    rows = jnp.zeros((8, values[0].shape[1]), f32)
    for i, value in enumerate(values):
        rows = jnp.where(at == i, value, rows)
    return rows


def multiply(flat_ref, j, weight, columns):
    twice = jnp.concatenate([weight, weight], axis=0)
    flat_ref[j] = lax.dot_general(twice, columns, (((0,), (0,)), ((), ())), preferred_element_type=f32)


def place(flat_ref, stage_ref, last, owners):
    count, width = flat_ref.shape[:2]
    size = width // stage_ref.shape[0]
    for i in owners:
        for j in range(count):
            stage_ref[i, j * size : (j + 1) * size] = flat_ref[j, i * size : (i + 1) * size]
        stage_ref[i, count * size : count * size + last.shape[0]] = last


def gain_lanes(gains):
    lane = lax.broadcasted_iota(jnp.int32, (gains[0].shape[0], 128), 1)
    lanes = jnp.zeros(lane.shape, f32)
    for i, rest in enumerate(gains):
        for k in range(3):
            part = rest.astype(bf16).astype(f32)
            lanes = jnp.where(lane == 3 * i + k, part, lanes)
            rest = rest - part
    return lanes.astype(bf16)


def gain_of(lanes, i):
    lane = lax.broadcasted_iota(jnp.int32, lanes.shape, 1)
    return jnp.sum(jnp.where(lane // 3 == i, lanes.astype(f32), 0.0), axis=1, keepdims=True)


def first_kernel(*refs):
    sources, (out_ref, keep_out_ref, give_out_ref, *refs) = refs[:6], refs[6:]
    flat_ref, stage_ref, tiles_ref, keep_ref, give_ref, turn_ref, *held, in_sems, out_sems = refs
    pieces = [*sources[:3], sources[3].at[0], sources[4].at[0], *[source.at[1] for source in sources[3:]]]
    copies = [pltpu.make_async_copy(pieces[i], held[i], in_sems.at[i]) for i in range(8)]
    for copy in copies:
        copy.start()
    tokens_ref, pre_ref, post_ref, gate_ref, up_ref, *traded_refs = held
    for copy in copies[:3]:
        copy.wait()
    start = tokens_ref[...].astype(f32)
    squares = total(start * start)
    high = squares.astype(bf16).astype(f32)
    sums = rows_of([high, squares - high])[:4]
    columns = stacked(start * column(pre_ref[0:1]))
    for k, ref in enumerate((gate_ref, up_ref)):
        copies[3 + k].wait()
        multiply(flat_ref, k, ref[...], columns)
    n, groups = tiles_ref.shape[0], out_sems.shape[0] - 2
    writes = []
    for g in range(groups):
        part = slice(g * n // groups, (g + 1) * n // groups)
        place(flat_ref, stage_ref, sums, range(part.start, part.stop))
        tiles_ref[part] = stage_ref[part].astype(bf16)
        writes.append(pltpu.make_async_copy(tiles_ref.at[part], out_ref.at[part], out_sems.at[g]))
        writes[-1].start()

    low = lax.axis_index("y_low") == lax.axis_index("y_high")
    width, wide = traded_refs[0].shape[1], turn_ref.shape[1]
    half, step = width // 2, wide // 2
    for k, ref in enumerate(traded_refs):
        copies[5 + k].wait()
        turn_ref[:, :width] = ref[...].astype(f32)
        first, second = turn_ref[:, :half], pltpu.roll(turn_ref[...], wide - half, 1)[:, :half]
        keep_ref[:, k * step : k * step + half] = jnp.where(low, first, second).astype(bf16)
        give_ref[:, k * step : k * step + half] = jnp.where(low, second, first).astype(bf16)
    ntok = tokens_ref.shape[1]
    gains = gain_lanes([column(row) for row in (pre_ref[1:2], post_ref[0:1], post_ref[1:2])])
    for ref in (keep_ref, give_ref):
        ref[:, 3 * step : 3 * step + ntok] = tokens_ref[...]
        ref[:, 3 * step + ntok :] = gains
    for i, (source, target) in enumerate(((keep_ref, keep_out_ref), (give_ref, give_out_ref))):
        writes.append(pltpu.make_async_copy(source, target, out_sems.at[groups + i]))
        writes[-1].start()
    for write in writes:
        write.wait()


def first_tiles(n, *operands):
    (count, ntok), width = operands[0].shape, operands[-1].shape[2]
    rows, groups, step = 2 * (width // n) + 4, 2, -(-width // 256) * 128
    outs = [jax.ShapeDtypeStruct(shape, bf16) for shape in ((n, rows, ntok), *[(count, 3 * step + ntok + 128)] * 2)]
    hbm = pl.BlockSpec(memory_space=pltpu.HBM)
    return pl.pallas_call(
        first_kernel,
        out_shape=outs,
        in_specs=[hbm] * 6,
        out_specs=[hbm] * 3,
        scratch_shapes=[
            pltpu.VMEM((2, width, ntok), f32),
            pltpu.VMEM((n, rows, ntok), f32),
            *[pltpu.VMEM(out.shape, bf16) for out in outs],
            pltpu.VMEM((count, 2 * step), f32),
            *[pltpu.VMEM(x.shape, x.dtype) for x in operands[:3]],
            *[pltpu.VMEM((count, width), bf16) for _ in range(5)],
            pltpu.SemaphoreType.DMA((8,)),
            pltpu.SemaphoreType.DMA((groups + 2,)),
        ],
    )(*operands)


def second_kernel(*refs):
    branch_ref, mine_ref, side_ref, other_ref, out_ref, start_ref, gained_ref, last_ref, flat_ref, stage_ref = refs
    width, ntok = gained_ref.shape
    held, step = flat_ref.shape[1], mine_ref.shape[1] // 3
    sides = side_ref[...], other_ref[:, 3 * step :]
    start = jnp.concatenate([side[:, :ntok] for side in sides]).astype(f32)
    start_ref[...] = start[:width]
    gains = [jnp.concatenate([gain_of(side[:, ntok:], i) for side in sides]) for i in range(3)]
    branch = branch_ref[...]
    gained = branch * gains[1]
    gained_ref[...] = gained[:width]
    last_ref[...] = jnp.broadcast_to(gains[2][:width], gained_ref.shape)
    sums = [total(branch * branch), total(gained * gained), total(start * gained)]
    high = [part.astype(bf16).astype(f32) for part in sums]
    sums = rows_of(high + [part - rounded for part, rounded in zip(sums, high)])
    for i, columns in enumerate((gained, start)):
        columns = stacked(columns * gains[0])
        for k in range(2):
            weight = jnp.concatenate([ref[:, k * step : k * step + held] for ref in (mine_ref, other_ref)])
            multiply(flat_ref, 2 * i + k, weight, columns)
    place(flat_ref, stage_ref, sums, range(out_ref.shape[0]))
    out_ref[...] = stage_ref[...].astype(bf16)


def second_tiles(n, held, *operands):
    width, ntok = operands[1].shape[0], operands[0].shape[1]
    rows = 4 * (held // n) + 8
    vmem = pl.BlockSpec(memory_space=pltpu.VMEM)
    return pl.pallas_call(
        second_kernel,
        out_shape=[jax.ShapeDtypeStruct((n, rows, ntok), bf16), *[jax.ShapeDtypeStruct((width, ntok), f32)] * 3],
        in_specs=[vmem] * len(operands),
        out_specs=[vmem] * 4,
        scratch_shapes=[pltpu.VMEM((4, held, ntok), f32), pltpu.VMEM((n, rows, ntok), f32)],
        compiler_params=pltpu.CompilerParams(vmem_limit_bytes=12 * 2**20),
    )(*operands)


def traded(array):
    return lax.ppermute(array, "y_low", [(0, 1), (1, 0)])


def sublayers(tokens, pre_gain, post_gain, gate_weight, up_weight, down_weight):
    n = lax.axis_size(RA)
    size = gate_weight.shape[2] // n
    turned = tokens.T
    width, ntok = turned.shape
    low = lax.axis_index("y_low") == 0

    def pair(first, second):
        return jnp.where(low, first, second), jnp.where(low, second, first)

    held = gate_weight.shape[2] // 2
    down_weight = down_weight.transpose(0, 2, 1)
    tiles, keep, give = first_tiles(n, turned, pre_gain, post_gain, gate_weight, up_weight, down_weight)
    down_now = jnp.where(low, down_weight[0], down_weight[0] * 1)
    tiles, low, down_now = lax.optimization_barrier((tiles, low, down_now))
    other = traded(give)
    got = exchange(tiles, RA)
    step = -(-held // 128) * 128
    got, keep, side = lax.optimization_barrier((got, keep[:, : 3 * step], keep[:, 3 * step :]))
    got = jnp.sum(got.astype(f32), axis=0)
    squares = total(got[2 * size : 2 * size + 2])
    scale_in = lax.rsqrt(squares / D + EPSILON)

    def hidden_of(both, groups):
        hidden = (jax.nn.silu(both[:size]) * both[size:]).astype(bf16)
        return to_all(hidden, RA, groups).reshape(-1, ntok)

    hidden = hidden_of(got[: 2 * size] * scale_in, None)
    parts = decoded(to_all(coded(down_project(down_now, hidden)), SUM))
    branch = jnp.concatenate(pair(*jnp.sum(parts.reshape(2, -1, width, ntok), axis=1)))

    tiles, start, gained, last = second_tiles(n // 2, held, branch, keep, side, other)
    got = jnp.sum(exchange(tiles, RA, PARTS).astype(f32), axis=0)
    sums = got[4 * size : 4 * size + 3] + got[4 * size + 3 : 4 * size + 6]
    branch_sq, gained_sq, cross = sums[0:1], sums[1:2], sums[2:3]
    scale_out = lax.rsqrt(branch_sq / D + EPSILON)
    squares = RESIDUAL * RESIDUAL * squares + 2.0 * RESIDUAL * scale_out * cross + scale_out * scale_out * gained_sq
    scale_in = lax.rsqrt(squares / D + EPSILON)
    stream = RESIDUAL * start + gained * scale_out

    both = (RESIDUAL * got[2 * size : 4 * size] + scale_out * got[: 2 * size]) * scale_in
    hidden = hidden_of(both, PARTS)
    halves = pair(*[coded(down_project(x[:, 2 * step : 2 * step + held], hidden)) for x in (keep, other)])
    members = lax.axis_size("cb")
    parts = jnp.concatenate([jnp.broadcast_to(half[None], (members, *half.shape)) for half in halves])
    branch = jnp.sum(decoded(exchange(parts, SUM)), axis=0)
    branch_sq = jnp.sum(to_all(total(branch * branch), RA), axis=0)
    scale_out = lax.rsqrt(branch_sq / D + EPSILON)
    stream = RESIDUAL * stream + branch * last * scale_out
    return stream.astype(bf16).T


def solution(mesh):
    split = Mesh(mesh.devices.reshape(8, 2, 2, mesh.shape["cb"]), ("z", "y_high", "y_low", "cb"))
    return jax.shard_map(
        sublayers,
        mesh=split,
        in_specs=(P(None, RA), P(None, RA), P(None, RA), P(None, RA, "cb"), P(None, RA, "cb"), P(None, "cb", RA)),
        out_specs=P(None, RA),
        check_vma=False,
    )
```

```python
import jax
import jax.numpy as jnp
from jax import lax
from jax.experimental import pallas as pl
from jax.experimental.pallas import tpu as pltpu
from jax.sharding import Mesh
from jax.sharding import PartitionSpec as P


D = 2048
EPSILON = 1e-06
RESIDUAL = 0.25
f32 = jnp.float32
bf16 = jnp.bfloat16
RA = ("z", "y_high", "y_low")
PARTS = [[4 * z + y for z in range(8) for y in ys] for ys in ((0, 3), (1, 2))]
SUM = ("y_low", "cb")


def exchange(tiles, axis, groups=None):
    return lax.all_to_all(tiles, axis, 0, 0, axis_index_groups=groups, tiled=True)


def to_all(tile, axis, groups=None):
    n = len(groups[0]) if groups else lax.axis_size(axis)
    return exchange(jnp.broadcast_to(tile[None], (n, *tile.shape)), axis, groups)


def coded(part):
    top = jnp.maximum(jnp.max(jnp.abs(part), axis=0, keepdims=True), 1e-30)
    power = jnp.floor(jnp.log2(top))
    return jnp.concatenate([part * jnp.exp2(-power), jnp.broadcast_to(power, (8, part.shape[1]))]).astype(jnp.float16)


def decoded(tiles):
    tiles = tiles.astype(f32)
    width = tiles.shape[1] - 8
    return tiles[:, :width] * jnp.exp2(tiles[:, width : width + 1])


def down_project(weight, columns):
    return jnp.dot(weight, columns, preferred_element_type=f32)


def total(sums):
    return jnp.sum(sums, axis=0, keepdims=True)


def column(row):
    k = row.shape[1]
    same = lax.broadcasted_iota(jnp.int32, (k, k), 0) == lax.broadcasted_iota(jnp.int32, (k, k), 1)
    return jnp.sum(jnp.where(same, row, 0.0), axis=1, keepdims=True)


def stacked(columns):
    high = columns.astype(bf16)
    return jnp.concatenate([high, (columns - high.astype(f32)).astype(bf16)], axis=0)


def rows_of(values):
    at = lax.broadcasted_iota(jnp.int32, (8, values[0].shape[1]), 0)
    rows = jnp.zeros((8, values[0].shape[1]), f32)
    for i, value in enumerate(values):
        rows = jnp.where(at == i, value, rows)
    return rows


def multiply(flat_ref, j, weight, columns):
    twice = jnp.concatenate([weight, weight], axis=0)
    flat_ref[j] = lax.dot_general(twice, columns, (((0,), (0,)), ((), ())), preferred_element_type=f32)


def place(flat_ref, stage_ref, last, owners):
    count, width = flat_ref.shape[:2]
    size = width // stage_ref.shape[0]
    for i in owners:
        for j in range(count):
            stage_ref[i, j * size : (j + 1) * size] = flat_ref[j, i * size : (i + 1) * size]
        stage_ref[i, count * size : count * size + last.shape[0]] = last


def gain_lanes(gains):
    lane = lax.broadcasted_iota(jnp.int32, (gains[0].shape[0], 128), 1)
    lanes = jnp.zeros(lane.shape, f32)
    for i, rest in enumerate(gains):
        for k in range(3):
            part = rest.astype(bf16).astype(f32)
            lanes = jnp.where(lane == 3 * i + k, part, lanes)
            rest = rest - part
    return lanes.astype(bf16)


def gain_of(lanes, i):
    lane = lax.broadcasted_iota(jnp.int32, lanes.shape, 1)
    return jnp.sum(jnp.where(lane // 3 == i, lanes.astype(f32), 0.0), axis=1, keepdims=True)


def first_kernel(*refs):
    sources, (out_ref, flat_ref, stage_ref, tiles_ref, *held, in_sems, out_sems) = refs[:4], refs[4:]
    pieces = [*sources[:2], sources[2].at[0], sources[3].at[0]]
    copies = [pltpu.make_async_copy(pieces[i], held[i], in_sems.at[i]) for i in range(4)]
    for copy in copies:
        copy.start()
    tokens_ref, pre_ref, gate_ref, up_ref = held
    for copy in copies[:2]:
        copy.wait()
    start = tokens_ref[...].astype(f32)
    squares = total(start * start)
    high = squares.astype(bf16).astype(f32)
    sums = rows_of([high, squares - high])[:4]
    columns = stacked(start * column(pre_ref[0:1]))
    for k, ref in enumerate((gate_ref, up_ref)):
        copies[2 + k].wait()
        multiply(flat_ref, k, ref[...], columns)
    n, groups = tiles_ref.shape[0], out_sems.shape[0]
    writes = []
    for g in range(groups):
        part = slice(g * n // groups, (g + 1) * n // groups)
        place(flat_ref, stage_ref, sums, range(part.start, part.stop))
        tiles_ref[part] = stage_ref[part].astype(bf16)
        writes.append(pltpu.make_async_copy(tiles_ref.at[part], out_ref.at[part], out_sems.at[g]))
        writes[-1].start()
    for write in writes:
        write.wait()


def first_tiles(n, *operands):
    (count, ntok), width = operands[0].shape, operands[-1].shape[2]
    rows, groups = 2 * (width // n) + 4, 2
    hbm = pl.BlockSpec(memory_space=pltpu.HBM)
    return pl.pallas_call(
        first_kernel,
        out_shape=jax.ShapeDtypeStruct((n, rows, ntok), bf16),
        in_specs=[hbm] * 4,
        out_specs=hbm,
        scratch_shapes=[
            pltpu.VMEM((2, width, ntok), f32),
            pltpu.VMEM((n, rows, ntok), f32),
            pltpu.VMEM((n, rows, ntok), bf16),
            *[pltpu.VMEM(x.shape, x.dtype) for x in operands[:2]],
            *[pltpu.VMEM((count, width), bf16) for _ in range(2)],
            pltpu.SemaphoreType.DMA((4,)),
            pltpu.SemaphoreType.DMA((groups,)),
        ],
    )(*operands)


def halves_kernel(*refs):
    sources, (keep_out_ref, give_out_ref, keep_ref, give_ref, turn_ref, *held, in_sems, out_sems) = refs[:6], refs[6:]
    pieces = [*sources[:3], *[source.at[1] for source in sources[3:]]]
    copies = [pltpu.make_async_copy(pieces[i], held[i], in_sems.at[i]) for i in range(6)]
    for copy in copies:
        copy.start()
    tokens_ref, pre_ref, post_ref, *traded_refs = held
    low = lax.axis_index("y_low") == lax.axis_index("y_high")
    width, wide = traded_refs[0].shape[1], turn_ref.shape[1]
    half, step, ntok = width // 2, wide // 2, tokens_ref.shape[1]
    for copy in copies:
        copy.wait()
    for k, ref in enumerate(traded_refs):
        turn_ref[:, :width] = ref[...].astype(f32)
        first, second = turn_ref[:, :half], pltpu.roll(turn_ref[...], wide - half, 1)[:, :half]
        keep_ref[:, k * step : k * step + half] = jnp.where(low, first, second).astype(bf16)
        give_ref[:, k * step : k * step + half] = jnp.where(low, second, first).astype(bf16)
    gains = gain_lanes([column(row) for row in (pre_ref[1:2], post_ref[0:1], post_ref[1:2])])
    for ref in (keep_ref, give_ref):
        ref[:, 3 * step : 3 * step + ntok] = tokens_ref[...]
        ref[:, 3 * step + ntok :] = gains
    writes = []
    for i, (source, target) in enumerate(((keep_ref, keep_out_ref), (give_ref, give_out_ref))):
        writes.append(pltpu.make_async_copy(source, target, out_sems.at[i]))
        writes[-1].start()
    for write in writes:
        write.wait()


def halves_of(*operands):
    (count, ntok), width = operands[0].shape, operands[-1].shape[2]
    step = -(-width // 256) * 128
    out = jax.ShapeDtypeStruct((count, 3 * step + ntok + 128), bf16)
    hbm = pl.BlockSpec(memory_space=pltpu.HBM)
    return pl.pallas_call(
        halves_kernel,
        out_shape=[out] * 2,
        in_specs=[hbm] * 6,
        out_specs=[hbm] * 2,
        scratch_shapes=[
            *[pltpu.VMEM(out.shape, bf16)] * 2,
            pltpu.VMEM((count, 2 * step), f32),
            *[pltpu.VMEM(x.shape, x.dtype) for x in operands[:3]],
            *[pltpu.VMEM((count, width), bf16) for _ in range(3)],
            pltpu.SemaphoreType.DMA((6,)),
            pltpu.SemaphoreType.DMA((2,)),
        ],
    )(*operands)


def second_kernel(*refs):
    branch_ref, mine_ref, side_ref, other_ref, out_ref, start_ref, gained_ref, last_ref, flat_ref, stage_ref = refs
    width, ntok = gained_ref.shape
    held, step = flat_ref.shape[1], mine_ref.shape[1] // 3
    sides = side_ref[...], other_ref[:, 3 * step :]
    start = jnp.concatenate([side[:, :ntok] for side in sides]).astype(f32)
    start_ref[...] = start[:width]
    gains = [jnp.concatenate([gain_of(side[:, ntok:], i) for side in sides]) for i in range(3)]
    branch = branch_ref[...]
    gained = branch * gains[1]
    gained_ref[...] = gained[:width]
    last_ref[...] = jnp.broadcast_to(gains[2][:width], gained_ref.shape)
    sums = [total(branch * branch), total(gained * gained), total(start * gained)]
    high = [part.astype(bf16).astype(f32) for part in sums]
    sums = rows_of(high + [part - rounded for part, rounded in zip(sums, high)])
    for i, columns in enumerate((gained, start)):
        columns = stacked(columns * gains[0])
        for k in range(2):
            weight = jnp.concatenate([ref[:, k * step : k * step + held] for ref in (mine_ref, other_ref)])
            multiply(flat_ref, 2 * i + k, weight, columns)
    place(flat_ref, stage_ref, sums, range(out_ref.shape[0]))
    out_ref[...] = stage_ref[...].astype(bf16)


def second_tiles(n, held, *operands):
    width, ntok = operands[1].shape[0], operands[0].shape[1]
    rows = 4 * (held // n) + 8
    vmem = pl.BlockSpec(memory_space=pltpu.VMEM)
    return pl.pallas_call(
        second_kernel,
        out_shape=[jax.ShapeDtypeStruct((n, rows, ntok), bf16), *[jax.ShapeDtypeStruct((width, ntok), f32)] * 3],
        in_specs=[vmem] * len(operands),
        out_specs=[vmem] * 4,
        scratch_shapes=[pltpu.VMEM((4, held, ntok), f32), pltpu.VMEM((n, rows, ntok), f32)],
        compiler_params=pltpu.CompilerParams(vmem_limit_bytes=12 * 2**20),
    )(*operands)


def traded(array):
    return lax.ppermute(array, "y_low", [(0, 1), (1, 0)])


def sublayers(tokens, pre_gain, post_gain, gate_weight, up_weight, down_weight):
    n = lax.axis_size(RA)
    size = gate_weight.shape[2] // n
    turned = tokens.T
    width, ntok = turned.shape
    low = lax.axis_index("y_low") == 0

    def pair(first, second):
        return jnp.where(low, first, second), jnp.where(low, second, first)

    held = gate_weight.shape[2] // 2
    down_weight = down_weight.transpose(0, 2, 1)
    tiles = first_tiles(n, turned, pre_gain, gate_weight, up_weight)
    tiles, low = lax.optimization_barrier((tiles, low))
    got = exchange(tiles, RA)
    keep, give = halves_of(turned, pre_gain, post_gain, gate_weight, up_weight, down_weight)
    other = traded(give)
    step = -(-held // 128) * 128
    got, keep, side, down_now = lax.optimization_barrier(
        (got, keep[:, : 3 * step], keep[:, 3 * step :], down_weight[0])
    )
    got = jnp.sum(got.astype(f32), axis=0)
    squares = total(got[2 * size : 2 * size + 2])
    scale_in = lax.rsqrt(squares / D + EPSILON)

    def hidden_of(both, groups):
        hidden = (jax.nn.silu(both[:size]) * both[size:]).astype(bf16)
        return to_all(hidden, RA, groups).reshape(-1, ntok)

    hidden = hidden_of(got[: 2 * size] * scale_in, None)
    parts = decoded(to_all(coded(down_project(down_now, hidden)), SUM))
    branch = jnp.concatenate(pair(*jnp.sum(parts.reshape(2, -1, width, ntok), axis=1)))

    tiles, start, gained, last = second_tiles(n // 2, held, branch, keep, side, other)
    got = jnp.sum(exchange(tiles, RA, PARTS).astype(f32), axis=0)
    sums = got[4 * size : 4 * size + 3] + got[4 * size + 3 : 4 * size + 6]
    branch_sq, gained_sq, cross = sums[0:1], sums[1:2], sums[2:3]
    scale_out = lax.rsqrt(branch_sq / D + EPSILON)
    squares = RESIDUAL * RESIDUAL * squares + 2.0 * RESIDUAL * scale_out * cross + scale_out * scale_out * gained_sq
    scale_in = lax.rsqrt(squares / D + EPSILON)
    stream = RESIDUAL * start + gained * scale_out

    both = (RESIDUAL * got[2 * size : 4 * size] + scale_out * got[: 2 * size]) * scale_in
    hidden = hidden_of(both, PARTS)
    halves = pair(*[coded(down_project(x[:, 2 * step : 2 * step + held], hidden)) for x in (keep, other)])
    members = lax.axis_size("cb")
    parts = jnp.concatenate([jnp.broadcast_to(half[None], (members, *half.shape)) for half in halves])
    branch = jnp.sum(decoded(exchange(parts, SUM)), axis=0)
    branch_sq = jnp.sum(to_all(total(branch * branch), RA), axis=0)
    scale_out = lax.rsqrt(branch_sq / D + EPSILON)
    stream = RESIDUAL * stream + branch * last * scale_out
    return stream.astype(bf16).T


def solution(mesh):
    split = Mesh(mesh.devices.reshape(8, 2, 2, mesh.shape["cb"]), ("z", "y_high", "y_low", "cb"))
    return jax.shard_map(
        sublayers,
        mesh=split,
        in_specs=(P(None, RA), P(None, RA), P(None, RA), P(None, RA, "cb"), P(None, RA, "cb"), P(None, "cb", RA)),
        out_specs=P(None, RA),
        check_vma=False,
    )
```

```python
import jax
import jax.numpy as jnp
from jax import lax
from jax.experimental import pallas as pl
from jax.experimental.pallas import tpu as pltpu
from jax.sharding import Mesh
from jax.sharding import PartitionSpec as P


D = 2048
EPSILON = 1e-06
RESIDUAL = 0.25
f32 = jnp.float32
bf16 = jnp.bfloat16
RA = ("z", "y_high", "y_low")
PARTS = [[4 * z + y for z in range(8) for y in ys] for ys in ((0, 3), (1, 2))]
SUM = ("y_low", "cb")


def exchange(tiles, axis, groups=None):
    return lax.all_to_all(tiles, axis, 0, 0, axis_index_groups=groups, tiled=True)


def to_all(tile, axis, groups=None):
    n = len(groups[0]) if groups else lax.axis_size(axis)
    return exchange(jnp.broadcast_to(tile[None], (n, *tile.shape)), axis, groups)


def coded(part):
    top = jnp.maximum(jnp.max(jnp.abs(part), axis=0, keepdims=True), 1e-30)
    power = jnp.floor(jnp.log2(top))
    return jnp.concatenate([part * jnp.exp2(-power), jnp.broadcast_to(power, (8, part.shape[1]))]).astype(jnp.float16)


def decoded(tiles):
    tiles = tiles.astype(f32)
    width = tiles.shape[1] - 8
    return tiles[:, :width] * jnp.exp2(tiles[:, width : width + 1])


def down_project(weight, columns):
    return jnp.dot(weight, columns, preferred_element_type=f32)


def total(sums):
    return jnp.sum(sums, axis=0, keepdims=True)


def column(row):
    k = row.shape[1]
    same = lax.broadcasted_iota(jnp.int32, (k, k), 0) == lax.broadcasted_iota(jnp.int32, (k, k), 1)
    return jnp.sum(jnp.where(same, row, 0.0), axis=1, keepdims=True)


def stacked(columns):
    high = columns.astype(bf16)
    return jnp.concatenate([high, (columns - high.astype(f32)).astype(bf16)], axis=0)


def rows_of(values):
    at = lax.broadcasted_iota(jnp.int32, (8, values[0].shape[1]), 0)
    rows = jnp.zeros((8, values[0].shape[1]), f32)
    for i, value in enumerate(values):
        rows = jnp.where(at == i, value, rows)
    return rows


def multiply(flat_ref, j, weight, columns):
    twice = jnp.concatenate([weight, weight], axis=0)
    flat_ref[j] = lax.dot_general(twice, columns, (((0,), (0,)), ((), ())), preferred_element_type=f32)


def place(flat_ref, stage_ref, last, owners):
    count, width = flat_ref.shape[:2]
    size = width // stage_ref.shape[0]
    for i in owners:
        for j in range(count):
            stage_ref[i, j * size : (j + 1) * size] = flat_ref[j, i * size : (i + 1) * size]
        stage_ref[i, count * size : count * size + last.shape[0]] = last


def gain_lanes(gains):
    lane = lax.broadcasted_iota(jnp.int32, (gains[0].shape[0], 128), 1)
    lanes = jnp.zeros(lane.shape, f32)
    for i, rest in enumerate(gains):
        for k in range(3):
            part = rest.astype(bf16).astype(f32)
            lanes = jnp.where(lane == 3 * i + k, part, lanes)
            rest = rest - part
    return lanes.astype(bf16)


def gain_of(lanes, i):
    lane = lax.broadcasted_iota(jnp.int32, lanes.shape, 1)
    return jnp.sum(jnp.where(lane // 3 == i, lanes.astype(f32), 0.0), axis=1, keepdims=True)


def first_kernel(*refs):
    sources, (out_ref, flat_ref, stage_ref, tiles_ref, *held, in_sems, out_sems) = refs[:4], refs[4:]
    pieces = [*sources[:2], sources[2].at[0], sources[3].at[0]]
    copies = [pltpu.make_async_copy(pieces[i], held[i], in_sems.at[i]) for i in range(4)]
    for copy in copies:
        copy.start()
    tokens_ref, pre_ref, gate_ref, up_ref = held
    for copy in copies[:2]:
        copy.wait()
    start = tokens_ref[...].astype(f32)
    squares = total(start * start)
    high = squares.astype(bf16).astype(f32)
    sums = rows_of([high, squares - high])[:4]
    columns = stacked(start * column(pre_ref[0:1]))
    for k, ref in enumerate((gate_ref, up_ref)):
        copies[2 + k].wait()
        multiply(flat_ref, k, ref[...], columns)
    n, groups = tiles_ref.shape[0], out_sems.shape[0]
    writes = []
    for g in range(groups):
        part = slice(g * n // groups, (g + 1) * n // groups)
        place(flat_ref, stage_ref, sums, range(part.start, part.stop))
        tiles_ref[part] = stage_ref[part].astype(bf16)
        writes.append(pltpu.make_async_copy(tiles_ref.at[part], out_ref.at[part], out_sems.at[g]))
        writes[-1].start()
    for write in writes:
        write.wait()


def first_tiles(n, *operands):
    (count, ntok), width = operands[0].shape, operands[-1].shape[2]
    rows, groups = 2 * (width // n) + 4, 2
    hbm = pl.BlockSpec(memory_space=pltpu.HBM)
    return pl.pallas_call(
        first_kernel,
        out_shape=jax.ShapeDtypeStruct((n, rows, ntok), bf16),
        in_specs=[hbm] * 4,
        out_specs=hbm,
        scratch_shapes=[
            pltpu.VMEM((2, width, ntok), f32),
            pltpu.VMEM((n, rows, ntok), f32),
            pltpu.VMEM((n, rows, ntok), bf16),
            *[pltpu.VMEM(x.shape, x.dtype) for x in operands[:2]],
            *[pltpu.VMEM((count, width), bf16) for _ in range(2)],
            pltpu.SemaphoreType.DMA((4,)),
            pltpu.SemaphoreType.DMA((groups,)),
        ],
    )(*operands)


def halves_kernel(*refs):
    sources, (keep_out_ref, give_out_ref, keep_ref, give_ref, turn_ref, *held, in_sems, out_sems) = refs[:5], refs[5:]
    pieces = [*sources[:3], *[source.at[1] for source in sources[3:]]]
    copies = [pltpu.make_async_copy(pieces[i], held[i], in_sems.at[i]) for i in range(5)]
    for copy in copies:
        copy.start()
    tokens_ref, pre_ref, post_ref, *traded_refs = held
    low = lax.axis_index("y_low") == lax.axis_index("y_high")
    width, wide = traded_refs[0].shape[1], turn_ref.shape[1]
    half, step, ntok = width // 2, wide // 2, tokens_ref.shape[1]
    for copy in copies:
        copy.wait()
    for k, ref in enumerate(traded_refs):
        turn_ref[:, :width] = ref[...].astype(f32)
        first, second = turn_ref[:, :half], pltpu.roll(turn_ref[...], wide - half, 1)[:, :half]
        keep_ref[:, k * step : k * step + half] = jnp.where(low, first, second).astype(bf16)
        give_ref[:, k * step : k * step + half] = jnp.where(low, second, first).astype(bf16)
    gains = gain_lanes([column(row) for row in (pre_ref[1:2], post_ref[0:1], post_ref[1:2])])
    for ref in (keep_ref, give_ref):
        ref[:, 2 * step : 2 * step + ntok] = tokens_ref[...]
        ref[:, 2 * step + ntok :] = gains
    writes = []
    for i, (source, target) in enumerate(((keep_ref, keep_out_ref), (give_ref, give_out_ref))):
        writes.append(pltpu.make_async_copy(source, target, out_sems.at[i]))
        writes[-1].start()
    for write in writes:
        write.wait()


def halves_of(*operands):
    (count, ntok), width = operands[0].shape, operands[-1].shape[2]
    step = -(-width // 256) * 128
    out = jax.ShapeDtypeStruct((count, 2 * step + ntok + 128), bf16)
    hbm = pl.BlockSpec(memory_space=pltpu.HBM)
    return pl.pallas_call(
        halves_kernel,
        out_shape=[out] * 2,
        in_specs=[hbm] * 5,
        out_specs=[hbm] * 2,
        scratch_shapes=[
            *[pltpu.VMEM(out.shape, bf16)] * 2,
            pltpu.VMEM((count, 2 * step), f32),
            *[pltpu.VMEM(x.shape, x.dtype) for x in operands[:3]],
            *[pltpu.VMEM((count, width), bf16) for _ in range(2)],
            pltpu.SemaphoreType.DMA((5,)),
            pltpu.SemaphoreType.DMA((2,)),
        ],
    )(*operands)


def second_kernel(*refs):
    branch_ref, mine_ref, side_ref, other_ref, out_ref, start_ref, gained_ref, last_ref, flat_ref, stage_ref = refs
    width, ntok = gained_ref.shape
    held, step = flat_ref.shape[1], mine_ref.shape[1] // 2
    sides = side_ref[...], other_ref[:, 2 * step :]
    start = jnp.concatenate([side[:, :ntok] for side in sides]).astype(f32)
    start_ref[...] = start[:width]
    gains = [jnp.concatenate([gain_of(side[:, ntok:], i) for side in sides]) for i in range(3)]
    branch = branch_ref[...]
    gained = branch * gains[1]
    gained_ref[...] = gained[:width]
    last_ref[...] = jnp.broadcast_to(gains[2][:width], gained_ref.shape)
    sums = [total(branch * branch), total(gained * gained), total(start * gained)]
    high = [part.astype(bf16).astype(f32) for part in sums]
    sums = rows_of(high + [part - rounded for part, rounded in zip(sums, high)])
    for i, columns in enumerate((gained, start)):
        columns = stacked(columns * gains[0])
        for k in range(2):
            weight = jnp.concatenate([ref[:, k * step : k * step + held] for ref in (mine_ref, other_ref)])
            multiply(flat_ref, 2 * i + k, weight, columns)
    place(flat_ref, stage_ref, sums, range(out_ref.shape[0]))
    out_ref[...] = stage_ref[...].astype(bf16)


def second_tiles(n, held, *operands):
    width, ntok = operands[1].shape[0], operands[0].shape[1]
    rows = 4 * (held // n) + 8
    vmem = pl.BlockSpec(memory_space=pltpu.VMEM)
    return pl.pallas_call(
        second_kernel,
        out_shape=[jax.ShapeDtypeStruct((n, rows, ntok), bf16), *[jax.ShapeDtypeStruct((width, ntok), f32)] * 3],
        in_specs=[vmem] * len(operands),
        out_specs=[vmem] * 4,
        scratch_shapes=[pltpu.VMEM((4, held, ntok), f32), pltpu.VMEM((n, rows, ntok), f32)],
        compiler_params=pltpu.CompilerParams(vmem_limit_bytes=12 * 2**20),
    )(*operands)


def traded(array):
    return lax.ppermute(array, "y_low", [(0, 1), (1, 0)])


def sublayers(tokens, pre_gain, post_gain, gate_weight, up_weight, down_weight):
    n = lax.axis_size(RA)
    size = gate_weight.shape[2] // n
    turned = tokens.T
    width, ntok = turned.shape
    low = lax.axis_index("y_low") == 0

    def pair(first, second):
        return jnp.where(low, first, second), jnp.where(low, second, first)

    held = gate_weight.shape[2] // 2
    down_weight = down_weight.transpose(0, 2, 1)
    tiles = first_tiles(n, turned, pre_gain, gate_weight, up_weight)
    tiles, low = lax.optimization_barrier((tiles, low))
    got = exchange(tiles, RA)
    keep, give = halves_of(turned, pre_gain, post_gain, gate_weight, up_weight)
    other = traded(give)
    step = -(-held // 128) * 128
    got, keep, side, down_now, down_next = lax.optimization_barrier(
        (got, keep[:, : 2 * step], keep[:, 2 * step :], down_weight[0], down_weight[1])
    )
    got = jnp.sum(got.astype(f32), axis=0)
    squares = total(got[2 * size : 2 * size + 2])
    scale_in = lax.rsqrt(squares / D + EPSILON)

    def hidden_of(both, groups):
        hidden = (jax.nn.silu(both[:size]) * both[size:]).astype(bf16)
        return to_all(hidden, RA, groups).reshape(-1, ntok)

    hidden = hidden_of(got[: 2 * size] * scale_in, None)
    parts = decoded(to_all(coded(down_project(down_now, hidden)), SUM))
    branch = jnp.concatenate(pair(*jnp.sum(parts.reshape(2, -1, width, ntok), axis=1)))

    tiles, start, gained, last = second_tiles(n // 2, held, branch, keep, side, other)
    got = jnp.sum(exchange(tiles, RA, PARTS).astype(f32), axis=0)
    sums = got[4 * size : 4 * size + 3] + got[4 * size + 3 : 4 * size + 6]
    branch_sq, gained_sq, cross = sums[0:1], sums[1:2], sums[2:3]
    scale_out = lax.rsqrt(branch_sq / D + EPSILON)
    squares = RESIDUAL * RESIDUAL * squares + 2.0 * RESIDUAL * scale_out * cross + scale_out * scale_out * gained_sq
    scale_in = lax.rsqrt(squares / D + EPSILON)
    stream = RESIDUAL * start + gained * scale_out

    both = (RESIDUAL * got[2 * size : 4 * size] + scale_out * got[: 2 * size]) * scale_in
    hidden = hidden_of(both, [PARTS[0] + PARTS[1]])
    branch = jnp.sum(decoded(to_all(coded(down_project(down_next, hidden)), "cb")), axis=0)
    branch_sq = jnp.sum(to_all(total(branch * branch), RA), axis=0)
    scale_out = lax.rsqrt(branch_sq / D + EPSILON)
    stream = RESIDUAL * stream + branch * last * scale_out
    return stream.astype(bf16).T


def solution(mesh):
    split = Mesh(mesh.devices.reshape(8, 2, 2, mesh.shape["cb"]), ("z", "y_high", "y_low", "cb"))
    return jax.shard_map(
        sublayers,
        mesh=split,
        in_specs=(P(None, RA), P(None, RA), P(None, RA), P(None, RA, "cb"), P(None, RA, "cb"), P(None, "cb", RA)),
        out_specs=P(None, RA),
        check_vma=False,
    )
```

```python
import jax
import jax.numpy as jnp
from jax import lax
from jax.experimental import pallas as pl
from jax.experimental.pallas import tpu as pltpu
from jax.sharding import Mesh
from jax.sharding import PartitionSpec as P


D = 2048
EPSILON = 1e-06
RESIDUAL = 0.25
f32 = jnp.float32
bf16 = jnp.bfloat16
RA = ("z", "y_high", "y_low")
PARTS = [[4 * z + y for z in range(8) for y in ys] for ys in ((0, 3), (1, 2))]
CB = ("chip", "core")


def exchange(tiles, axis, groups=None):
    return lax.all_to_all(tiles, axis, 0, 0, axis_index_groups=groups, tiled=True)


def to_all(tile, axis, groups=None):
    n = len(groups[0]) if groups else lax.axis_size(axis)
    return exchange(jnp.broadcast_to(tile[None], (n, *tile.shape)), axis, groups)


def coded(part):
    top = jnp.maximum(jnp.max(jnp.abs(part), axis=0, keepdims=True), 1e-30)
    power = jnp.floor(jnp.log2(top))
    return jnp.concatenate([part * jnp.exp2(-power), jnp.broadcast_to(power, (8, part.shape[1]))]).astype(jnp.float16)


def decoded(tiles):
    tiles = tiles.astype(f32)
    width = tiles.shape[1] - 8
    return tiles[:, :width] * jnp.exp2(tiles[:, width : width + 1])


def down_project(weight, columns):
    return jnp.dot(weight, columns, preferred_element_type=f32)


def total(sums):
    return jnp.sum(sums, axis=0, keepdims=True)


def column(row):
    k = row.shape[1]
    same = lax.broadcasted_iota(jnp.int32, (k, k), 0) == lax.broadcasted_iota(jnp.int32, (k, k), 1)
    return jnp.sum(jnp.where(same, row, 0.0), axis=1, keepdims=True)


def stacked(columns):
    high = columns.astype(bf16)
    return jnp.concatenate([high, (columns - high.astype(f32)).astype(bf16)], axis=0)


def rows_of(values):
    at = lax.broadcasted_iota(jnp.int32, (8, values[0].shape[1]), 0)
    rows = jnp.zeros((8, values[0].shape[1]), f32)
    for i, value in enumerate(values):
        rows = jnp.where(at == i, value, rows)
    return rows


def multiply(flat_ref, j, weight, columns):
    twice = jnp.concatenate([weight, weight], axis=0)
    flat_ref[j] = lax.dot_general(twice, columns, (((0,), (0,)), ((), ())), preferred_element_type=f32)


def place(flat_ref, stage_ref, last, owners):
    count, width = flat_ref.shape[:2]
    size = width // stage_ref.shape[0]
    for i in owners:
        for j in range(count):
            stage_ref[i, j * size : (j + 1) * size] = flat_ref[j, i * size : (i + 1) * size]
        stage_ref[i, count * size : count * size + last.shape[0]] = last


def gain_lanes(gains):
    lane = lax.broadcasted_iota(jnp.int32, (gains[0].shape[0], 128), 1)
    lanes = jnp.zeros(lane.shape, f32)
    for i, rest in enumerate(gains):
        for k in range(3):
            part = rest.astype(bf16).astype(f32)
            lanes = jnp.where(lane == 3 * i + k, part, lanes)
            rest = rest - part
    return lanes.astype(bf16)


def gain_of(lanes, i):
    lane = lax.broadcasted_iota(jnp.int32, lanes.shape, 1)
    return jnp.sum(jnp.where(lane // 3 == i, lanes.astype(f32), 0.0), axis=1, keepdims=True)


def first_kernel(*refs):
    sources, (out_ref, flat_ref, stage_ref, tiles_ref, *held, in_sems, out_sems) = refs[:4], refs[4:]
    pieces = [*sources[:2], sources[2].at[0], sources[3].at[0]]
    copies = [pltpu.make_async_copy(pieces[i], held[i], in_sems.at[i]) for i in range(4)]
    for copy in copies:
        copy.start()
    tokens_ref, pre_ref, gate_ref, up_ref = held
    for copy in copies[:2]:
        copy.wait()
    start = tokens_ref[...].astype(f32)
    squares = total(start * start)
    high = squares.astype(bf16).astype(f32)
    sums = rows_of([high, squares - high])[:4]
    columns = stacked(start * column(pre_ref[0:1]))
    for k, ref in enumerate((gate_ref, up_ref)):
        copies[2 + k].wait()
        multiply(flat_ref, k, ref[...], columns)
    n, groups = tiles_ref.shape[0], out_sems.shape[0]
    writes = []
    for g in range(groups):
        part = slice(g * n // groups, (g + 1) * n // groups)
        place(flat_ref, stage_ref, sums, range(part.start, part.stop))
        tiles_ref[part] = stage_ref[part].astype(bf16)
        writes.append(pltpu.make_async_copy(tiles_ref.at[part], out_ref.at[part], out_sems.at[g]))
        writes[-1].start()
    for write in writes:
        write.wait()


def first_tiles(n, *operands):
    (count, ntok), width = operands[0].shape, operands[-1].shape[2]
    rows, groups = 2 * (width // n) + 4, 2
    hbm = pl.BlockSpec(memory_space=pltpu.HBM)
    return pl.pallas_call(
        first_kernel,
        out_shape=jax.ShapeDtypeStruct((n, rows, ntok), bf16),
        in_specs=[hbm] * 4,
        out_specs=hbm,
        scratch_shapes=[
            pltpu.VMEM((2, width, ntok), f32),
            pltpu.VMEM((n, rows, ntok), f32),
            pltpu.VMEM((n, rows, ntok), bf16),
            *[pltpu.VMEM(x.shape, x.dtype) for x in operands[:2]],
            *[pltpu.VMEM((count, width), bf16) for _ in range(2)],
            pltpu.SemaphoreType.DMA((4,)),
            pltpu.SemaphoreType.DMA((groups,)),
        ],
    )(*operands)


def halves_kernel(*refs):
    sources, (keep_out_ref, give_out_ref, keep_ref, give_ref, turn_ref, *held, in_sems, out_sems) = refs[:5], refs[5:]
    pieces = [*sources[:3], *[source.at[1] for source in sources[3:]]]
    copies = [pltpu.make_async_copy(pieces[i], held[i], in_sems.at[i]) for i in range(5)]
    for copy in copies:
        copy.start()
    tokens_ref, pre_ref, post_ref, *traded_refs = held
    low = lax.axis_index("y_low") == lax.axis_index("y_high")
    width, wide = traded_refs[0].shape[1], turn_ref.shape[1]
    half, step, ntok = width // 2, wide // 2, tokens_ref.shape[1]
    for copy in copies:
        copy.wait()
    for k, ref in enumerate(traded_refs):
        turn_ref[:, :width] = ref[...].astype(f32)
        first, second = turn_ref[:, :half], pltpu.roll(turn_ref[...], wide - half, 1)[:, :half]
        keep_ref[:, k * step : k * step + half] = jnp.where(low, first, second).astype(bf16)
        give_ref[:, k * step : k * step + half] = jnp.where(low, second, first).astype(bf16)
    gains = gain_lanes([column(row) for row in (pre_ref[1:2], post_ref[0:1], post_ref[1:2])])
    for ref in (keep_ref, give_ref):
        ref[:, 2 * step : 2 * step + ntok] = tokens_ref[...]
        ref[:, 2 * step + ntok :] = gains
    writes = []
    for i, (source, target) in enumerate(((keep_ref, keep_out_ref), (give_ref, give_out_ref))):
        writes.append(pltpu.make_async_copy(source, target, out_sems.at[i]))
        writes[-1].start()
    for write in writes:
        write.wait()


def halves_of(*operands):
    (count, ntok), width = operands[0].shape, operands[-1].shape[2]
    step = -(-width // 256) * 128
    out = jax.ShapeDtypeStruct((count, 2 * step + ntok + 128), bf16)
    hbm = pl.BlockSpec(memory_space=pltpu.HBM)
    return pl.pallas_call(
        halves_kernel,
        out_shape=[out] * 2,
        in_specs=[hbm] * 5,
        out_specs=[hbm] * 2,
        scratch_shapes=[
            *[pltpu.VMEM(out.shape, bf16)] * 2,
            pltpu.VMEM((count, 2 * step), f32),
            *[pltpu.VMEM(x.shape, x.dtype) for x in operands[:3]],
            *[pltpu.VMEM((count, width), bf16) for _ in range(2)],
            pltpu.SemaphoreType.DMA((5,)),
            pltpu.SemaphoreType.DMA((2,)),
        ],
    )(*operands)


def second_kernel(*refs):
    branch_ref, mine_ref, side_ref, other_ref, out_ref, start_ref, gained_ref, last_ref, flat_ref, stage_ref = refs
    width, ntok = gained_ref.shape
    held, step = flat_ref.shape[1], mine_ref.shape[1] // 2
    sides = side_ref[...], other_ref[:, 2 * step :]
    start = jnp.concatenate([side[:, :ntok] for side in sides]).astype(f32)
    start_ref[...] = start[:width]
    gains = [jnp.concatenate([gain_of(side[:, ntok:], i) for side in sides]) for i in range(3)]
    branch = branch_ref[...]
    gained = branch * gains[1]
    gained_ref[...] = gained[:width]
    last_ref[...] = jnp.broadcast_to(gains[2][:width], gained_ref.shape)
    sums = [total(branch * branch), total(gained * gained), total(start * gained)]
    high = [part.astype(bf16).astype(f32) for part in sums]
    sums = rows_of(high + [part - rounded for part, rounded in zip(sums, high)])
    for i, columns in enumerate((gained, start)):
        columns = stacked(columns * gains[0])
        for k in range(2):
            weight = jnp.concatenate([ref[:, k * step : k * step + held] for ref in (mine_ref, other_ref)])
            multiply(flat_ref, 2 * i + k, weight, columns)
    place(flat_ref, stage_ref, sums, range(out_ref.shape[0]))
    out_ref[...] = stage_ref[...].astype(bf16)


def second_tiles(n, held, *operands):
    width, ntok = operands[1].shape[0], operands[0].shape[1]
    rows = 4 * (held // n) + 8
    vmem = pl.BlockSpec(memory_space=pltpu.VMEM)
    return pl.pallas_call(
        second_kernel,
        out_shape=[jax.ShapeDtypeStruct((n, rows, ntok), bf16), *[jax.ShapeDtypeStruct((width, ntok), f32)] * 3],
        in_specs=[vmem] * len(operands),
        out_specs=[vmem] * 4,
        scratch_shapes=[pltpu.VMEM((4, held, ntok), f32), pltpu.VMEM((n, rows, ntok), f32)],
        compiler_params=pltpu.CompilerParams(vmem_limit_bytes=12 * 2**20),
    )(*operands)


def traded(array):
    return lax.ppermute(array, "y_low", [(0, 1), (1, 0)])


def sublayers(tokens, pre_gain, post_gain, gate_weight, up_weight, down_weight):
    n = lax.axis_size(RA)
    size = gate_weight.shape[2] // n
    turned = tokens.T
    width, ntok = turned.shape
    low = lax.axis_index("y_low") == 0

    def pair(first, second):
        return jnp.where(low, first, second), jnp.where(low, second, first)

    held = gate_weight.shape[2] // 2
    down_weight = down_weight.transpose(0, 2, 1)
    tiles = first_tiles(n, turned, pre_gain, gate_weight, up_weight)
    tiles, low = lax.optimization_barrier((tiles, low))
    got = exchange(tiles, RA)
    keep, give = halves_of(turned, pre_gain, post_gain, gate_weight, up_weight)
    other = traded(give)
    step = -(-held // 128) * 128
    got, keep, side, down_now, down_next = lax.optimization_barrier(
        (got, keep[:, : 2 * step], keep[:, 2 * step :], down_weight[0], down_weight[1])
    )
    got = jnp.sum(got.astype(f32), axis=0)
    squares = total(got[2 * size : 2 * size + 2])
    scale_in = lax.rsqrt(squares / D + EPSILON)

    def hidden_of(both, groups):
        hidden = (jax.nn.silu(both[:size]) * both[size:]).astype(bf16)
        return to_all(hidden, RA, groups).reshape(-1, ntok)

    hidden = hidden_of(got[: 2 * size] * scale_in, None)
    part = down_project(down_now, hidden)
    part = part + lax.ppermute(part, "core", [(0, 1), (1, 0)])
    parts = decoded(to_all(coded(part), ("y_low", "chip")))
    branch = jnp.concatenate(pair(*jnp.sum(parts.reshape(2, -1, width, ntok), axis=1)))

    tiles, start, gained, last = second_tiles(n // 2, held, branch, keep, side, other)
    got = jnp.sum(exchange(tiles, RA, PARTS).astype(f32), axis=0)
    sums = got[4 * size : 4 * size + 3] + got[4 * size + 3 : 4 * size + 6]
    branch_sq, gained_sq, cross = sums[0:1], sums[1:2], sums[2:3]
    scale_out = lax.rsqrt(branch_sq / D + EPSILON)
    squares = RESIDUAL * RESIDUAL * squares + 2.0 * RESIDUAL * scale_out * cross + scale_out * scale_out * gained_sq
    scale_in = lax.rsqrt(squares / D + EPSILON)
    stream = RESIDUAL * start + gained * scale_out

    both = (RESIDUAL * got[2 * size : 4 * size] + scale_out * got[: 2 * size]) * scale_in
    hidden = hidden_of(both, [PARTS[0] + PARTS[1]])
    branch = jnp.sum(decoded(to_all(coded(down_project(down_next, hidden)), CB)), axis=0)
    branch_sq = jnp.sum(to_all(total(branch * branch), RA), axis=0)
    scale_out = lax.rsqrt(branch_sq / D + EPSILON)
    stream = RESIDUAL * stream + branch * last * scale_out
    return stream.astype(bf16).T


def solution(mesh):
    split = Mesh(mesh.devices.reshape(8, 2, 2, mesh.shape["cb"] // 2, 2), ("z", "y_high", "y_low", "chip", "core"))
    return jax.shard_map(
        sublayers,
        mesh=split,
        in_specs=(P(None, RA), P(None, RA), P(None, RA), P(None, RA, CB), P(None, RA, CB), P(None, CB, RA)),
        out_specs=P(None, RA),
        check_vma=False,
    )
```

```python
import jax
import jax.numpy as jnp
from jax import lax
from jax.experimental import pallas as pl
from jax.experimental.pallas import tpu as pltpu
from jax.sharding import Mesh
from jax.sharding import PartitionSpec as P


D = 2048
EPSILON = 1e-06
RESIDUAL = 0.25
f32 = jnp.float32
bf16 = jnp.bfloat16
RA = ("z", "y")
CB = ("chip", "core")


def exchange(tiles, axis, groups=None):
    return lax.all_to_all(tiles, axis, 0, 0, axis_index_groups=groups, tiled=True)


def to_all(tile, axis, groups=None):
    n = len(groups[0]) if groups else lax.axis_size(axis)
    return exchange(jnp.broadcast_to(tile[None], (n, *tile.shape)), axis, groups)


def coded(part):
    top = jnp.maximum(jnp.max(jnp.abs(part), axis=0, keepdims=True), 1e-30)
    power = jnp.floor(jnp.log2(top))
    return jnp.concatenate([part * jnp.exp2(-power), jnp.broadcast_to(power, (8, part.shape[1]))]).astype(jnp.float16)


def decoded(tiles):
    tiles = tiles.astype(f32)
    width = tiles.shape[1] - 8
    return tiles[:, :width] * jnp.exp2(tiles[:, width : width + 1])


def down_project(weight, columns):
    return jnp.dot(weight, columns, preferred_element_type=f32)


def total(sums):
    return jnp.sum(sums, axis=0, keepdims=True)


def column(row):
    k = row.shape[1]
    same = lax.broadcasted_iota(jnp.int32, (k, k), 0) == lax.broadcasted_iota(jnp.int32, (k, k), 1)
    return jnp.sum(jnp.where(same, row, 0.0), axis=1, keepdims=True)


def stacked(columns):
    high = columns.astype(bf16)
    return jnp.concatenate([high, (columns - high.astype(f32)).astype(bf16)], axis=0)


def rows_of(values):
    at = lax.broadcasted_iota(jnp.int32, (8, values[0].shape[1]), 0)
    rows = jnp.zeros((8, values[0].shape[1]), f32)
    for i, value in enumerate(values):
        rows = jnp.where(at == i, value, rows)
    return rows


def multiply(flat_ref, j, weight, columns):
    twice = jnp.concatenate([weight, weight], axis=0)
    flat_ref[j] = lax.dot_general(twice, columns, (((0,), (0,)), ((), ())), preferred_element_type=f32)


def place(flat_ref, stage_ref, last, owners):
    count, width = flat_ref.shape[:2]
    size = width // stage_ref.shape[0]
    for i in owners:
        for j in range(count):
            stage_ref[i, j * size : (j + 1) * size] = flat_ref[j, i * size : (i + 1) * size]
        stage_ref[i, count * size : count * size + last.shape[0]] = last


def gain_lanes(gains):
    lane = lax.broadcasted_iota(jnp.int32, (gains[0].shape[0], 128), 1)
    lanes = jnp.zeros(lane.shape, f32)
    for i, rest in enumerate(gains):
        for k in range(3):
            part = rest.astype(bf16).astype(f32)
            lanes = jnp.where(lane == 3 * i + k, part, lanes)
            rest = rest - part
    return lanes.astype(bf16)


def gain_of(lanes, i):
    lane = lax.broadcasted_iota(jnp.int32, lanes.shape, 1)
    return jnp.sum(jnp.where(lane // 3 == i, lanes.astype(f32), 0.0), axis=1, keepdims=True)


def first_kernel(*refs):
    sources, (out_ref, flat_ref, stage_ref, tiles_ref, *held, in_sems, out_sems) = refs[:4], refs[4:]
    pieces = [*sources[:2], sources[2].at[0], sources[3].at[0]]
    copies = [pltpu.make_async_copy(pieces[i], held[i], in_sems.at[i]) for i in range(4)]
    for copy in copies:
        copy.start()
    tokens_ref, pre_ref, gate_ref, up_ref = held
    for copy in copies[:2]:
        copy.wait()
    start = tokens_ref[...].astype(f32)
    squares = total(start * start)
    high = squares.astype(bf16).astype(f32)
    sums = rows_of([high, squares - high])[:4]
    columns = stacked(start * column(pre_ref[0:1]))
    for k, ref in enumerate((gate_ref, up_ref)):
        copies[2 + k].wait()
        multiply(flat_ref, k, ref[...], columns)
    n, groups = tiles_ref.shape[0], out_sems.shape[0]
    writes = []
    for g in range(groups):
        part = slice(g * n // groups, (g + 1) * n // groups)
        place(flat_ref, stage_ref, sums, range(part.start, part.stop))
        tiles_ref[part] = stage_ref[part].astype(bf16)
        writes.append(pltpu.make_async_copy(tiles_ref.at[part], out_ref.at[part], out_sems.at[g]))
        writes[-1].start()
    for write in writes:
        write.wait()


def first_tiles(n, *operands):
    (count, ntok), width = operands[0].shape, operands[-1].shape[2]
    rows, groups = 2 * (width // n) + 4, 2
    hbm = pl.BlockSpec(memory_space=pltpu.HBM)
    return pl.pallas_call(
        first_kernel,
        out_shape=jax.ShapeDtypeStruct((n, rows, ntok), bf16),
        in_specs=[hbm] * 4,
        out_specs=hbm,
        scratch_shapes=[
            pltpu.VMEM((2, width, ntok), f32),
            pltpu.VMEM((n, rows, ntok), f32),
            pltpu.VMEM((n, rows, ntok), bf16),
            *[pltpu.VMEM(x.shape, x.dtype) for x in operands[:2]],
            *[pltpu.VMEM((count, width), bf16) for _ in range(2)],
            pltpu.SemaphoreType.DMA((4,)),
            pltpu.SemaphoreType.DMA((groups,)),
        ],
    )(*operands)


def quarters_kernel(*refs):
    sources, outs, (parts_ref, turn_ref, *held, in_sems, out_sems) = refs[:5], refs[5:9], refs[9:]
    pieces = [*sources[:3], *[source.at[1] for source in sources[3:]]]
    copies = [pltpu.make_async_copy(pieces[i], held[i], in_sems.at[i]) for i in range(5)]
    for copy in copies:
        copy.start()
    tokens_ref, pre_ref, post_ref, *traded_refs = held
    place_y = lax.axis_index("y")
    width, wide = traded_refs[0].shape[1], turn_ref.shape[1]
    quarter, step, ntok = width // 4, (parts_ref.shape[2] - 256) // 2, tokens_ref.shape[1]
    for copy in copies:
        copy.wait()
    for k, ref in enumerate(traded_refs):
        turn_ref[:, :width] = ref[...].astype(f32)
        quarters = [turn_ref[:, :quarter]]
        quarters += [pltpu.roll(turn_ref[...], wide - i * quarter, 1)[:, :quarter] for i in range(1, 4)]
        for d in range(4):
            part = quarters[d]
            for y in range(1, 4):
                part = jnp.where(place_y == y, quarters[(y + d) % 4], part)
            parts_ref[d, :, k * step : k * step + quarter] = part.astype(bf16)
    gains = gain_lanes([column(row) for row in (pre_ref[1:2], post_ref[0:1], post_ref[1:2])])
    for d in range(4):
        parts_ref[d, :, 2 * step : 2 * step + ntok] = tokens_ref[...]
        parts_ref[d, :, 2 * step + ntok :] = gains
    writes = [pltpu.make_async_copy(parts_ref.at[d], outs[d], out_sems.at[d]) for d in range(4)]
    for write in writes:
        write.start()
    for write in writes:
        write.wait()


def quarters_of(*operands):
    (count, ntok), width = operands[0].shape, operands[-1].shape[2]
    step = -(-width // 512) * 128
    out = jax.ShapeDtypeStruct((count, 2 * step + ntok + 128), bf16)
    hbm = pl.BlockSpec(memory_space=pltpu.HBM)
    return pl.pallas_call(
        quarters_kernel,
        out_shape=[out] * 4,
        in_specs=[hbm] * 5,
        out_specs=[hbm] * 4,
        scratch_shapes=[
            pltpu.VMEM((4, *out.shape), bf16),
            pltpu.VMEM((count, -(-width // 128) * 128), f32),
            *[pltpu.VMEM(x.shape, x.dtype) for x in operands[:3]],
            *[pltpu.VMEM((count, width), bf16) for _ in range(2)],
            pltpu.SemaphoreType.DMA((5,)),
            pltpu.SemaphoreType.DMA((4,)),
        ],
    )(*operands)


def second_kernel(*refs):
    branch_ref, mine_ref, side_ref, *other_refs = refs[:6]
    out_ref, start_ref, gained_ref, last_ref, flat_ref, stage_ref = refs[6:]
    width, ntok = gained_ref.shape
    held, step = flat_ref.shape[1], mine_ref.shape[1] // 2
    sides = [side_ref[...], *[ref[:, 2 * step :] for ref in other_refs]]
    start = jnp.concatenate([side[:, :ntok] for side in sides]).astype(f32)
    start_ref[...] = start[:width]
    gains = [jnp.concatenate([gain_of(side[:, ntok:], i) for side in sides]) for i in range(3)]
    branch = branch_ref[...]
    gained = branch * gains[1]
    gained_ref[...] = gained[:width]
    last_ref[...] = jnp.broadcast_to(gains[2][:width], gained_ref.shape)
    sums = [total(branch * branch), total(gained * gained), total(start * gained)]
    high = [part.astype(bf16).astype(f32) for part in sums]
    sums = rows_of(high + [part - rounded for part, rounded in zip(sums, high)])
    for i, columns in enumerate((gained, start)):
        columns = stacked(columns * gains[0])
        for k in range(2):
            weight = jnp.concatenate([ref[:, k * step : k * step + held] for ref in (mine_ref, *other_refs)])
            multiply(flat_ref, 2 * i + k, weight, columns)
    place(flat_ref, stage_ref, sums, range(out_ref.shape[0]))
    out_ref[...] = stage_ref[...].astype(bf16)


def second_tiles(n, held, *operands):
    width, ntok = operands[1].shape[0], operands[0].shape[1]
    rows = 4 * (held // n) + 8
    vmem = pl.BlockSpec(memory_space=pltpu.VMEM)
    return pl.pallas_call(
        second_kernel,
        out_shape=[jax.ShapeDtypeStruct((n, rows, ntok), bf16), *[jax.ShapeDtypeStruct((width, ntok), f32)] * 3],
        in_specs=[vmem] * len(operands),
        out_specs=[vmem] * 4,
        scratch_shapes=[pltpu.VMEM((4, held, ntok), f32), pltpu.VMEM((n, rows, ntok), f32)],
        compiler_params=pltpu.CompilerParams(vmem_limit_bytes=12 * 2**20),
    )(*operands)


def handed(array, d):
    return lax.ppermute(array, "y", [(i, (i + d) % 4) for i in range(4)])


def sublayers(tokens, pre_gain, post_gain, gate_weight, up_weight, down_weight):
    n = lax.axis_size(RA)
    size = gate_weight.shape[2] // n
    turned = tokens.T
    width, ntok = turned.shape
    held = gate_weight.shape[2] // 4
    down_weight = down_weight.transpose(0, 2, 1)
    turn = ((4 - lax.axis_index("y")) % 4).astype(jnp.uint32)
    tiles = first_tiles(n, turned, pre_gain, gate_weight, up_weight)
    tiles, turn = lax.optimization_barrier((tiles, turn))
    got = exchange(tiles, RA)
    keep, *gives = quarters_of(turned, pre_gain, post_gain, gate_weight, up_weight)
    others = []
    for d, give in enumerate(gives, 1):
        others.append(handed(give, d))
    step = -(-held // 128) * 128
    got, keep, side, down_now, down_next = lax.optimization_barrier(
        (got, keep[:, : 2 * step], keep[:, 2 * step :], down_weight[0], down_weight[1])
    )
    got = jnp.sum(got.astype(f32), axis=0)
    squares = total(got[2 * size : 2 * size + 2])
    scale_in = lax.rsqrt(squares / D + EPSILON)

    def hidden_of(both, groups):
        hidden = (jax.nn.silu(both[:size]) * both[size:]).astype(bf16)
        return to_all(hidden, RA, groups).reshape(-1, ntok)

    hidden = hidden_of(got[: 2 * size] * scale_in, None)
    part = down_project(down_now, hidden)
    part = part + lax.ppermute(part, "core", [(0, 1), (1, 0)])
    parts = decoded(to_all(coded(part), ("y", "chip")))
    parts = jnp.sum(parts.reshape(4, -1, width, ntok), axis=1)
    parts = jnp.stack([parts[-i % 4] for i in range(8)])
    branch = lax.dynamic_slice_in_dim(parts, turn, 4).reshape(4 * width, ntok)

    tiles, start, gained, last = second_tiles(lax.axis_size("z"), held, branch, keep, side, *others)
    got = jnp.sum(exchange(tiles, "z").astype(f32), axis=0)
    sums = got[4 * size : 4 * size + 3] + got[4 * size + 3 : 4 * size + 6]
    branch_sq, gained_sq, cross = sums[0:1], sums[1:2], sums[2:3]
    scale_out = lax.rsqrt(branch_sq / D + EPSILON)
    squares = RESIDUAL * RESIDUAL * squares + 2.0 * RESIDUAL * scale_out * cross + scale_out * scale_out * gained_sq
    scale_in = lax.rsqrt(squares / D + EPSILON)
    stream = RESIDUAL * start + gained * scale_out

    both = (RESIDUAL * got[2 * size : 4 * size] + scale_out * got[: 2 * size]) * scale_in
    hidden = hidden_of(both, [[4 * z + y for y in range(4) for z in range(8)]])
    branch = jnp.sum(decoded(to_all(coded(down_project(down_next, hidden)), CB)), axis=0)
    branch_sq = jnp.sum(to_all(total(branch * branch), RA), axis=0)
    scale_out = lax.rsqrt(branch_sq / D + EPSILON)
    stream = RESIDUAL * stream + branch * last * scale_out
    return stream.astype(bf16).T


def solution(mesh):
    split = Mesh(mesh.devices.reshape(8, 4, mesh.shape["cb"] // 2, 2), ("z", "y", "chip", "core"))
    return jax.shard_map(
        sublayers,
        mesh=split,
        in_specs=(P(None, RA), P(None, RA), P(None, RA), P(None, RA, CB), P(None, RA, CB), P(None, CB, RA)),
        out_specs=P(None, RA),
        check_vma=False,
    )
```

```python
import jax
import jax.numpy as jnp
from jax import lax
from jax.experimental import pallas as pl
from jax.experimental.pallas import tpu as pltpu
from jax.sharding import Mesh
from jax.sharding import PartitionSpec as P


D = 2048
EPSILON = 1e-06
RESIDUAL = 0.25
f32 = jnp.float32
bf16 = jnp.bfloat16
RA = ("z", "y")
CB = ("chip", "core")


def exchange(tiles, axis, groups=None):
    return lax.all_to_all(tiles, axis, 0, 0, axis_index_groups=groups, tiled=True)


def to_all(tile, axis, groups=None):
    n = len(groups[0]) if groups else lax.axis_size(axis)
    return exchange(jnp.broadcast_to(tile[None], (n, *tile.shape)), axis, groups)


def coded(part):
    top = jnp.maximum(jnp.max(jnp.abs(part), axis=0, keepdims=True), 1e-30)
    power = jnp.floor(jnp.log2(top))
    return jnp.concatenate([part * jnp.exp2(-power), jnp.broadcast_to(power, (8, part.shape[1]))]).astype(jnp.float16)


def decoded(tiles):
    tiles = tiles.astype(f32)
    width = tiles.shape[1] - 8
    return tiles[:, :width] * jnp.exp2(tiles[:, width : width + 1])


def down_project(weight, columns):
    return jnp.dot(weight, columns, preferred_element_type=f32)


def total(sums):
    return jnp.sum(sums, axis=0, keepdims=True)


def column(row):
    k = row.shape[1]
    same = lax.broadcasted_iota(jnp.int32, (k, k), 0) == lax.broadcasted_iota(jnp.int32, (k, k), 1)
    return jnp.sum(jnp.where(same, row, 0.0), axis=1, keepdims=True)


def stacked(columns):
    high = columns.astype(bf16)
    return jnp.concatenate([high, (columns - high.astype(f32)).astype(bf16)], axis=0)


def rows_of(values):
    at = lax.broadcasted_iota(jnp.int32, (8, values[0].shape[1]), 0)
    rows = jnp.zeros((8, values[0].shape[1]), f32)
    for i, value in enumerate(values):
        rows = jnp.where(at == i, value, rows)
    return rows


def multiply(flat_ref, j, weight, columns):
    twice = jnp.concatenate([weight, weight], axis=0)
    flat_ref[j] = lax.dot_general(twice, columns, (((0,), (0,)), ((), ())), preferred_element_type=f32)


def place(flat_ref, stage_ref, last, owners):
    count, width = flat_ref.shape[:2]
    size = width // stage_ref.shape[0]
    for i in owners:
        rows = [flat_ref[j, i * size : (i + 1) * size] for j in range(count)]
        stage_ref[i] = jnp.concatenate([*rows, last]).astype(bf16)


def gain_lanes(gains):
    lane = lax.broadcasted_iota(jnp.int32, (gains[0].shape[0], 128), 1)
    lanes = jnp.zeros(lane.shape, f32)
    for i, rest in enumerate(gains):
        for k in range(3):
            part = rest.astype(bf16).astype(f32)
            lanes = jnp.where(lane == 3 * i + k, part, lanes)
            rest = rest - part
    return lanes.astype(bf16)


def gain_of(lanes, i):
    lane = lax.broadcasted_iota(jnp.int32, lanes.shape, 1)
    return jnp.sum(jnp.where(lane // 3 == i, lanes.astype(f32), 0.0), axis=1, keepdims=True)


def first_kernel(*refs):
    sources, (out_ref, flat_ref, tiles_ref, *held, in_sems, out_sems) = refs[:4], refs[4:]
    pieces = [*sources[:2], sources[2].at[0], sources[3].at[0]]
    copies = [pltpu.make_async_copy(pieces[i], held[i], in_sems.at[i]) for i in range(4)]
    for copy in copies:
        copy.start()
    tokens_ref, pre_ref, gate_ref, up_ref = held
    for copy in copies[:2]:
        copy.wait()
    start = tokens_ref[...].astype(f32)
    squares = total(start * start)
    high = squares.astype(bf16).astype(f32)
    sums = rows_of([high, squares - high])[:4]
    columns = stacked(start * column(pre_ref[0:1]))
    for k, ref in enumerate((gate_ref, up_ref)):
        copies[2 + k].wait()
        multiply(flat_ref, k, ref[...], columns)
    n, groups = tiles_ref.shape[0], out_sems.shape[0]
    writes = []
    for g in range(groups):
        part = slice(g * n // groups, (g + 1) * n // groups)
        place(flat_ref, tiles_ref, sums, range(part.start, part.stop))
        writes.append(pltpu.make_async_copy(tiles_ref.at[part], out_ref.at[part], out_sems.at[g]))
        writes[-1].start()
    for write in writes:
        write.wait()


def first_tiles(n, *operands):
    (count, ntok), width = operands[0].shape, operands[-1].shape[2]
    rows, groups = 2 * (width // n) + 4, 2
    hbm = pl.BlockSpec(memory_space=pltpu.HBM)
    return pl.pallas_call(
        first_kernel,
        out_shape=jax.ShapeDtypeStruct((n, rows, ntok), bf16),
        in_specs=[hbm] * 4,
        out_specs=hbm,
        scratch_shapes=[
            pltpu.VMEM((2, width, ntok), f32),
            pltpu.VMEM((n, rows, ntok), bf16),
            *[pltpu.VMEM(x.shape, x.dtype) for x in operands[:2]],
            *[pltpu.VMEM((count, width), bf16) for _ in range(2)],
            pltpu.SemaphoreType.DMA((4,)),
            pltpu.SemaphoreType.DMA((groups,)),
        ],
    )(*operands)


def quarters_kernel(*refs):
    sources, outs, (parts_ref, turn_ref, *held, in_sems, out_sems) = refs[:5], refs[5:9], refs[9:]
    pieces = [*sources[:3], *[source.at[1] for source in sources[3:]]]
    copies = [pltpu.make_async_copy(pieces[i], held[i], in_sems.at[i]) for i in range(5)]
    for copy in copies:
        copy.start()
    tokens_ref, pre_ref, post_ref, *traded_refs = held
    place_y = lax.axis_index("y")
    width, wide = traded_refs[0].shape[1], turn_ref.shape[1]
    quarter, step, ntok = width // 4, (parts_ref.shape[2] - 256) // 2, tokens_ref.shape[1]
    for copy in copies:
        copy.wait()
    for k, ref in enumerate(traded_refs):
        turn_ref[:, :width] = ref[...].astype(f32)
        quarters = [turn_ref[:, :quarter]]
        quarters += [pltpu.roll(turn_ref[...], wide - i * quarter, 1)[:, :quarter] for i in range(1, 4)]
        for d in range(4):
            part = quarters[d]
            for y in range(1, 4):
                part = jnp.where(place_y == y, quarters[(y + d) % 4], part)
            parts_ref[d, :, k * step : k * step + quarter] = part.astype(bf16)
    gains = gain_lanes([column(row) for row in (pre_ref[1:2], post_ref[0:1], post_ref[1:2])])
    for d in range(4):
        parts_ref[d, :, 2 * step : 2 * step + ntok] = tokens_ref[...]
        parts_ref[d, :, 2 * step + ntok :] = gains
    writes = [pltpu.make_async_copy(parts_ref.at[d], outs[d], out_sems.at[d]) for d in range(4)]
    for write in writes:
        write.start()
    for write in writes:
        write.wait()


def quarters_of(*operands):
    (count, ntok), width = operands[0].shape, operands[-1].shape[2]
    step = -(-width // 512) * 128
    out = jax.ShapeDtypeStruct((count, 2 * step + ntok + 128), bf16)
    hbm = pl.BlockSpec(memory_space=pltpu.HBM)
    return pl.pallas_call(
        quarters_kernel,
        out_shape=[out] * 4,
        in_specs=[hbm] * 5,
        out_specs=[hbm] * 4,
        scratch_shapes=[
            pltpu.VMEM((4, *out.shape), bf16),
            pltpu.VMEM((count, -(-width // 128) * 128), f32),
            *[pltpu.VMEM(x.shape, x.dtype) for x in operands[:3]],
            *[pltpu.VMEM((count, width), bf16) for _ in range(2)],
            pltpu.SemaphoreType.DMA((5,)),
            pltpu.SemaphoreType.DMA((4,)),
        ],
    )(*operands)


def second_kernel(*refs):
    branch_ref, mine_ref, side_ref, *other_refs = refs[:6]
    out_ref, start_ref, gained_ref, last_ref, flat_ref = refs[6:]
    width, ntok = gained_ref.shape
    held, step = flat_ref.shape[1], mine_ref.shape[1] // 2
    sides = [side_ref[...], *[ref[:, 2 * step :] for ref in other_refs]]
    start = jnp.concatenate([side[:, :ntok] for side in sides]).astype(f32)
    start_ref[...] = start[:width]
    gains = [jnp.concatenate([gain_of(side[:, ntok:], i) for side in sides]) for i in range(3)]
    branch = branch_ref[...]
    gained = branch * gains[1]
    gained_ref[...] = gained[:width]
    last_ref[...] = jnp.broadcast_to(gains[2][:width], gained_ref.shape)
    sums = [total(branch * branch), total(gained * gained), total(start * gained)]
    high = [part.astype(bf16).astype(f32) for part in sums]
    sums = rows_of(high + [part - rounded for part, rounded in zip(sums, high)])
    for i, columns in enumerate((gained, start)):
        columns = stacked(columns * gains[0])
        for k in range(2):
            weight = jnp.concatenate([ref[:, k * step : k * step + held] for ref in (mine_ref, *other_refs)])
            multiply(flat_ref, 2 * i + k, weight, columns)
    place(flat_ref, out_ref, sums, range(out_ref.shape[0]))


def second_tiles(n, held, *operands):
    width, ntok = operands[1].shape[0], operands[0].shape[1]
    rows = 4 * (held // n) + 8
    vmem = pl.BlockSpec(memory_space=pltpu.VMEM)
    return pl.pallas_call(
        second_kernel,
        out_shape=[jax.ShapeDtypeStruct((n, rows, ntok), bf16), *[jax.ShapeDtypeStruct((width, ntok), f32)] * 3],
        in_specs=[vmem] * len(operands),
        out_specs=[vmem] * 4,
        scratch_shapes=[pltpu.VMEM((4, held, ntok), f32)],
        compiler_params=pltpu.CompilerParams(vmem_limit_bytes=12 * 2**20),
    )(*operands)


def handed(array, d):
    return lax.ppermute(array, "y", [(i, (i + d) % 4) for i in range(4)])


def sublayers(tokens, pre_gain, post_gain, gate_weight, up_weight, down_weight):
    n = lax.axis_size(RA)
    size = gate_weight.shape[2] // n
    turned = tokens.T
    width, ntok = turned.shape
    held = gate_weight.shape[2] // 4
    down_weight = down_weight.transpose(0, 2, 1)
    turn = ((4 - lax.axis_index("y")) % 4).astype(jnp.uint32)
    tiles = first_tiles(n, turned, pre_gain, gate_weight, up_weight)
    tiles, turn = lax.optimization_barrier((tiles, turn))
    got = exchange(tiles, RA)
    keep, *gives = quarters_of(turned, pre_gain, post_gain, gate_weight, up_weight)
    others = []
    for d, give in enumerate(gives, 1):
        others.append(handed(give, d))
    step = -(-held // 128) * 128
    got, keep, side, down_now, down_next = lax.optimization_barrier(
        (got, keep[:, : 2 * step], keep[:, 2 * step :], down_weight[0], down_weight[1])
    )
    got = jnp.sum(got.astype(f32), axis=0)
    squares = total(got[2 * size : 2 * size + 2])
    scale_in = lax.rsqrt(squares / D + EPSILON)

    def hidden_of(both, groups):
        hidden = (jax.nn.silu(both[:size]) * both[size:]).astype(bf16)
        return to_all(hidden, RA, groups).reshape(-1, ntok)

    hidden = hidden_of(got[: 2 * size] * scale_in, None)
    part = down_project(down_now, hidden)
    part = part + lax.ppermute(part, "core", [(0, 1), (1, 0)])
    parts = decoded(to_all(coded(part), ("chip", "y")))
    parts = jnp.sum(parts.reshape(-1, 4, width, ntok), axis=0)
    parts = jnp.stack([parts[-i % 4] for i in range(8)])
    branch = lax.dynamic_slice_in_dim(parts, turn, 4).reshape(4 * width, ntok)

    tiles, start, gained, last = second_tiles(lax.axis_size("z"), held, branch, keep, side, *others)
    got = jnp.sum(exchange(tiles, "z").astype(f32), axis=0)
    sums = got[4 * size : 4 * size + 3] + got[4 * size + 3 : 4 * size + 6]
    branch_sq, gained_sq, cross = sums[0:1], sums[1:2], sums[2:3]
    scale_out = lax.rsqrt(branch_sq / D + EPSILON)
    squares = RESIDUAL * RESIDUAL * squares + 2.0 * RESIDUAL * scale_out * cross + scale_out * scale_out * gained_sq
    scale_in = lax.rsqrt(squares / D + EPSILON)
    stream = RESIDUAL * start + gained * scale_out

    both = (RESIDUAL * got[2 * size : 4 * size] + scale_out * got[: 2 * size]) * scale_in
    hidden = hidden_of(both, [[4 * z + y for y in range(4) for z in range(8)]])
    branch = jnp.sum(decoded(to_all(coded(down_project(down_next, hidden)), CB)), axis=0)
    branch_sq = jnp.sum(to_all(total(branch * branch), RA), axis=0)
    scale_out = lax.rsqrt(branch_sq / D + EPSILON)
    stream = RESIDUAL * stream + branch * last * scale_out
    return stream.astype(bf16).T


def solution(mesh):
    split = Mesh(mesh.devices.reshape(8, 4, mesh.shape["cb"] // 2, 2), ("z", "y", "chip", "core"))
    return jax.shard_map(
        sublayers,
        mesh=split,
        in_specs=(P(None, RA), P(None, RA), P(None, RA), P(None, RA, CB), P(None, RA, CB), P(None, CB, RA)),
        out_specs=P(None, RA),
        check_vma=False,
    )
```

```python
import jax
import jax.numpy as jnp
from jax import lax
from jax.experimental import pallas as pl
from jax.experimental.pallas import tpu as pltpu
from jax.sharding import Mesh
from jax.sharding import PartitionSpec as P


D = 2048
EPSILON = 1e-06
RESIDUAL = 0.25
f32 = jnp.float32
bf16 = jnp.bfloat16
RA = ("z", "y")
CB = ("chip", "core")


def exchange(tiles, axis, groups=None):
    return lax.all_to_all(tiles, axis, 0, 0, axis_index_groups=groups, tiled=True)


def to_all(tile, axis, groups=None):
    n = len(groups[0]) if groups else lax.axis_size(axis)
    return exchange(jnp.broadcast_to(tile[None], (n, *tile.shape)), axis, groups)


def coded(part):
    top = jnp.maximum(jnp.max(jnp.abs(part), axis=0, keepdims=True), 1e-30)
    power = jnp.floor(jnp.log2(top))
    return jnp.concatenate([part * jnp.exp2(-power), jnp.broadcast_to(power, (8, part.shape[1]))]).astype(jnp.float16)


def decoded(tiles):
    tiles = tiles.astype(f32)
    width = tiles.shape[1] - 8
    return tiles[:, :width] * jnp.exp2(tiles[:, width : width + 1])


def down_project(weight, columns):
    return jnp.dot(weight, columns, preferred_element_type=f32)


def total(sums):
    return jnp.sum(sums, axis=0, keepdims=True)


def column(row):
    k = row.shape[1]
    same = lax.broadcasted_iota(jnp.int32, (k, k), 0) == lax.broadcasted_iota(jnp.int32, (k, k), 1)
    return jnp.sum(jnp.where(same, row, 0.0), axis=1, keepdims=True)


def stacked(columns):
    high = columns.astype(bf16)
    return jnp.concatenate([high, (columns - high.astype(f32)).astype(bf16)], axis=0)


def rows_of(values):
    at = lax.broadcasted_iota(jnp.int32, (8, values[0].shape[1]), 0)
    rows = jnp.zeros((8, values[0].shape[1]), f32)
    for i, value in enumerate(values):
        rows = jnp.where(at == i, value, rows)
    return rows


def multiply(flat_ref, j, weight, columns):
    twice = jnp.concatenate([weight, weight], axis=0)
    flat_ref[j] = lax.dot_general(twice, columns, (((0,), (0,)), ((), ())), preferred_element_type=f32)


def place(flat_ref, stage_ref, last, owners):
    count, width = flat_ref.shape[:2]
    size = width // stage_ref.shape[0]
    for i in owners:
        for j in range(count):
            stage_ref[i, j * size : (j + 1) * size] = flat_ref[j, i * size : (i + 1) * size]
        stage_ref[i, count * size : count * size + last.shape[0]] = last


def gain_lanes(gains):
    lane = lax.broadcasted_iota(jnp.int32, (gains[0].shape[0], 128), 1)
    lanes = jnp.zeros(lane.shape, f32)
    for i, rest in enumerate(gains):
        for k in range(3):
            part = rest.astype(bf16).astype(f32)
            lanes = jnp.where(lane == 3 * i + k, part, lanes)
            rest = rest - part
    return lanes.astype(bf16)


def gain_of(lanes, i):
    lane = lax.broadcasted_iota(jnp.int32, lanes.shape, 1)
    return jnp.sum(jnp.where(lane // 3 == i, lanes.astype(f32), 0.0), axis=1, keepdims=True)


def first_kernel(*refs):
    sources, (out_ref, flat_ref, stage_ref, tiles_ref, *held, in_sems, out_sems) = refs[:4], refs[4:]
    pieces = [*sources[:2], sources[2].at[0], sources[3].at[0]]
    copies = [pltpu.make_async_copy(pieces[i], held[i], in_sems.at[i]) for i in range(4)]
    for copy in copies:
        copy.start()
    tokens_ref, pre_ref, gate_ref, up_ref = held
    for copy in copies[:2]:
        copy.wait()
    start = tokens_ref[...].astype(f32)
    squares = total(start * start)
    high = squares.astype(bf16).astype(f32)
    sums = rows_of([high, squares - high])[:4]
    columns = stacked(start * column(pre_ref[0:1]))
    for k, ref in enumerate((gate_ref, up_ref)):
        copies[2 + k].wait()
        multiply(flat_ref, k, ref[...], columns)
    n, groups = tiles_ref.shape[0], out_sems.shape[0]
    writes = []
    for g in range(groups):
        part = slice(g * n // groups, (g + 1) * n // groups)
        place(flat_ref, stage_ref, sums, range(part.start, part.stop))
        tiles_ref[part] = stage_ref[part].astype(bf16)
        writes.append(pltpu.make_async_copy(tiles_ref.at[part], out_ref.at[part], out_sems.at[g]))
        writes[-1].start()
    for write in writes:
        write.wait()


def first_tiles(n, *operands):
    (count, ntok), width = operands[0].shape, operands[-1].shape[2]
    rows, groups = 2 * (width // n) + 4, 4
    hbm = pl.BlockSpec(memory_space=pltpu.HBM)
    return pl.pallas_call(
        first_kernel,
        out_shape=jax.ShapeDtypeStruct((n, rows, ntok), bf16),
        in_specs=[hbm] * 4,
        out_specs=hbm,
        scratch_shapes=[
            pltpu.VMEM((2, width, ntok), f32),
            pltpu.VMEM((n, rows, ntok), f32),
            pltpu.VMEM((n, rows, ntok), bf16),
            *[pltpu.VMEM(x.shape, x.dtype) for x in operands[:2]],
            *[pltpu.VMEM((count, width), bf16) for _ in range(2)],
            pltpu.SemaphoreType.DMA((4,)),
            pltpu.SemaphoreType.DMA((groups,)),
        ],
    )(*operands)


def quarters_kernel(*refs):
    sources, outs, (parts_ref, turn_ref, *held, in_sems, out_sems) = refs[:5], refs[5:9], refs[9:]
    pieces = [*sources[:3], *[source.at[1] for source in sources[3:]]]
    copies = [pltpu.make_async_copy(pieces[i], held[i], in_sems.at[i]) for i in range(5)]
    for copy in copies:
        copy.start()
    tokens_ref, pre_ref, post_ref, *traded_refs = held
    place_y = lax.axis_index("y")
    width, wide = traded_refs[0].shape[1], turn_ref.shape[1]
    quarter, step, ntok = width // 4, (parts_ref.shape[2] - 256) // 2, tokens_ref.shape[1]
    for copy in copies:
        copy.wait()
    for k, ref in enumerate(traded_refs):
        turn_ref[:, :width] = ref[...].astype(f32)
        quarters = [turn_ref[:, :quarter]]
        quarters += [pltpu.roll(turn_ref[...], wide - i * quarter, 1)[:, :quarter] for i in range(1, 4)]
        for d in range(4):
            part = quarters[d]
            for y in range(1, 4):
                part = jnp.where(place_y == y, quarters[(y + d) % 4], part)
            parts_ref[d, :, k * step : k * step + quarter] = part.astype(bf16)
    gains = gain_lanes([column(row) for row in (pre_ref[1:2], post_ref[0:1], post_ref[1:2])])
    for d in range(4):
        parts_ref[d, :, 2 * step : 2 * step + ntok] = tokens_ref[...]
        parts_ref[d, :, 2 * step + ntok :] = gains
    writes = [pltpu.make_async_copy(parts_ref.at[d], outs[d], out_sems.at[d]) for d in range(4)]
    for write in writes:
        write.start()
    for write in writes:
        write.wait()


def quarters_of(*operands):
    (count, ntok), width = operands[0].shape, operands[-1].shape[2]
    step = -(-width // 512) * 128
    out = jax.ShapeDtypeStruct((count, 2 * step + ntok + 128), bf16)
    hbm = pl.BlockSpec(memory_space=pltpu.HBM)
    return pl.pallas_call(
        quarters_kernel,
        out_shape=[out] * 4,
        in_specs=[hbm] * 5,
        out_specs=[hbm] * 4,
        scratch_shapes=[
            pltpu.VMEM((4, *out.shape), bf16),
            pltpu.VMEM((count, -(-width // 128) * 128), f32),
            *[pltpu.VMEM(x.shape, x.dtype) for x in operands[:3]],
            *[pltpu.VMEM((count, width), bf16) for _ in range(2)],
            pltpu.SemaphoreType.DMA((5,)),
            pltpu.SemaphoreType.DMA((4,)),
        ],
    )(*operands)


def second_kernel(*refs):
    branch_ref, mine_ref, side_ref, *other_refs = refs[:6]
    out_ref, start_ref, gained_ref, last_ref, flat_ref, stage_ref = refs[6:]
    width, ntok = gained_ref.shape
    held, step = flat_ref.shape[1], mine_ref.shape[1] // 2
    sides = [side_ref[...], *[ref[:, 2 * step :] for ref in other_refs]]
    start = jnp.concatenate([side[:, :ntok] for side in sides]).astype(f32)
    start_ref[...] = start[:width]
    gains = [jnp.concatenate([gain_of(side[:, ntok:], i) for side in sides]) for i in range(3)]
    branch = branch_ref[...]
    gained = branch * gains[1]
    gained_ref[...] = gained[:width]
    last_ref[...] = jnp.broadcast_to(gains[2][:width], gained_ref.shape)
    sums = [total(branch * branch), total(gained * gained), total(start * gained)]
    high = [part.astype(bf16).astype(f32) for part in sums]
    sums = rows_of(high + [part - rounded for part, rounded in zip(sums, high)])
    for i, columns in enumerate((gained, start)):
        columns = stacked(columns * gains[0])
        for k in range(2):
            weight = jnp.concatenate([ref[:, k * step : k * step + held] for ref in (mine_ref, *other_refs)])
            multiply(flat_ref, 2 * i + k, weight, columns)
    place(flat_ref, stage_ref, sums, range(out_ref.shape[0]))
    out_ref[...] = stage_ref[...].astype(bf16)


def second_tiles(n, held, *operands):
    width, ntok = operands[1].shape[0], operands[0].shape[1]
    rows = 4 * (held // n) + 8
    vmem = pl.BlockSpec(memory_space=pltpu.VMEM)
    return pl.pallas_call(
        second_kernel,
        out_shape=[jax.ShapeDtypeStruct((n, rows, ntok), bf16), *[jax.ShapeDtypeStruct((width, ntok), f32)] * 3],
        in_specs=[vmem] * len(operands),
        out_specs=[vmem] * 4,
        scratch_shapes=[pltpu.VMEM((4, held, ntok), f32), pltpu.VMEM((n, rows, ntok), f32)],
        compiler_params=pltpu.CompilerParams(vmem_limit_bytes=12 * 2**20),
    )(*operands)


def handed(array, d):
    return lax.ppermute(array, "y", [(i, (i + d) % 4) for i in range(4)])


def sublayers(tokens, pre_gain, post_gain, gate_weight, up_weight, down_weight):
    n = lax.axis_size(RA)
    size = gate_weight.shape[2] // n
    turned = tokens.T
    width, ntok = turned.shape
    held = gate_weight.shape[2] // 4
    down_weight = down_weight.transpose(0, 2, 1)
    turn = ((4 - lax.axis_index("y")) % 4).astype(jnp.uint32)
    tiles = first_tiles(n, turned, pre_gain, gate_weight, up_weight)
    tiles, turn = lax.optimization_barrier((tiles, turn))
    got = exchange(tiles, RA)
    keep, *gives = quarters_of(turned, pre_gain, post_gain, gate_weight, up_weight)
    others = []
    for d, give in enumerate(gives, 1):
        others.append(handed(give, d))
    step = -(-held // 128) * 128
    got, keep, side, down_now, down_next = lax.optimization_barrier(
        (got, keep[:, : 2 * step], keep[:, 2 * step :], down_weight[0], down_weight[1])
    )
    got = jnp.sum(got.astype(f32), axis=0)
    squares = total(got[2 * size : 2 * size + 2])
    scale_in = lax.rsqrt(squares / D + EPSILON)

    def hidden_of(both, groups):
        hidden = (jax.nn.silu(both[:size]) * both[size:]).astype(bf16)
        return to_all(hidden, RA, groups).reshape(-1, ntok)

    hidden = hidden_of(got[: 2 * size] * scale_in, None)
    part = down_project(down_now, hidden)
    part = part + lax.ppermute(part, "core", [(0, 1), (1, 0)])
    parts = decoded(to_all(coded(part), ("chip", "y")))
    parts = jnp.sum(parts.reshape(-1, 4, width, ntok), axis=0)
    parts = jnp.stack([parts[-i % 4] for i in range(8)])
    branch = lax.dynamic_slice_in_dim(parts, turn, 4).reshape(4 * width, ntok)

    tiles, start, gained, last = second_tiles(lax.axis_size("z"), held, branch, keep, side, *others)
    got = jnp.sum(exchange(tiles, "z").astype(f32), axis=0)
    sums = got[4 * size : 4 * size + 3] + got[4 * size + 3 : 4 * size + 6]
    branch_sq, gained_sq, cross = sums[0:1], sums[1:2], sums[2:3]
    scale_out = lax.rsqrt(branch_sq / D + EPSILON)
    squares = RESIDUAL * RESIDUAL * squares + 2.0 * RESIDUAL * scale_out * cross + scale_out * scale_out * gained_sq
    scale_in = lax.rsqrt(squares / D + EPSILON)
    stream = RESIDUAL * start + gained * scale_out

    both = (RESIDUAL * got[2 * size : 4 * size] + scale_out * got[: 2 * size]) * scale_in
    hidden = hidden_of(both, [[4 * z + y for y in range(4) for z in range(8)]])
    branch = jnp.sum(decoded(to_all(coded(down_project(down_next, hidden)), CB)), axis=0)
    branch_sq = jnp.sum(to_all(total(branch * branch), RA), axis=0)
    scale_out = lax.rsqrt(branch_sq / D + EPSILON)
    stream = RESIDUAL * stream + branch * last * scale_out
    return stream.astype(bf16).T


def solution(mesh):
    split = Mesh(mesh.devices.reshape(8, 4, mesh.shape["cb"] // 2, 2), ("z", "y", "chip", "core"))
    return jax.shard_map(
        sublayers,
        mesh=split,
        in_specs=(P(None, RA), P(None, RA), P(None, RA), P(None, RA, CB), P(None, RA, CB), P(None, CB, RA)),
        out_specs=P(None, RA),
        check_vma=False,
    )
```
